32 devices in a mesh: ep: 4 (over y, x), tp: 8 (over z, core).
Axes of the slice: x: 2, y: 2, z: 4, core: 2. Of those that a mesh axis runs over, the one named last changes fastest.
Arguments:
- query_heads_rows: bfloat16 [2048, 2048], P('ep', 'tp'), may hold values from -9 to 9
- key_heads_rows: bfloat16 [2048, 2048], P('ep', 'tp'), may hold values from -9 to 9
- value_heads_rows: bfloat16 [2048, 2048], P('ep', 'tp'), may hold values from -6 to 6
- write_strength_logit: bfloat16 [16, 2048], P('tp', 'ep'), may hold values from -3.5 to -1
- decay_preactivation: bfloat16 [16, 2048], P('tp', 'ep'), may hold values from -5 to 5
- head_decay_logarithm: float32 [16], P('tp'), may hold values from -20 to -3
- extra_log_decay: float32 [16, 2048], P('tp', 'ep'), may hold values from -0.7 to 0
- output_weight: bfloat16 [2048, 2048], P('tp'), may hold values from -2 to 2
- second_batch_tokens: bfloat16 [4096, 2048], P(('ep', 'tp')), may hold values from -6 to 6
- expert_norm_scale: float32 [2048], replicated, may hold values from 0.1 to 1.9
- expert_choice_index: int32 [4096, 2], P(('ep', 'tp')), may hold values from 0 to 15, as said below
- group_router_weight: float32 [4096], P(('ep', 'tp')), may hold values from 0.25 to 1
- expert_logit_difference: float32 [4096], P(('ep', 'tp')), may hold values from -8 to 8
- expert_gate_weight: bfloat16 [16, 1024, 2048], P('ep', 'tp'), may hold values from -0.125 to 0.125
- expert_up_weight: bfloat16 [16, 1024, 2048], P('ep', 'tp'), may hold values from -0.125 to 0.125
- expert_down_weight: bfloat16 [16, 1024, 2048], P('ep', 'tp'), may hold values from -0.375 to 0.375
Outputs:
- mixer_output_first: bfloat16 [2048, 2048], P(('ep', 'tp'))
- expert_out: bfloat16 [4096, 2048], P(('ep', 'tp'))
The draws below stay inside these ranges and needn't reach their ends.
Inputs may be any that keep to these rules, and one draw needn't show every extreme that they name: `expert_choice_index`: each row names two different experts of one group, the experts a * 4 to a * 4 + 3 for some a. In the rows of one device (aligned blocks of 128 rows) no expert is named more than 32 times, and in every device's rows some expert is named exactly 32 times.
All inputs are finite; a program needn't handle non-finite values.
Results may differ from the reference program's by a relative error of at most 0.018.
Values may be sent and summed in bfloat16 or wider, within the bound.
No kernel may reach another device: no remote copies, remote signals or barrier semaphores. Data moves between devices by JAX's collectives and lax.ppermute only.
A program may use at most 128 MiB of HBM per device.

```python
import jax
import jax.numpy as jnp
from jax import lax

D = 2048
HEADS = 16
DK = 128
DV = 128
BLOCK = 64
TOK_AEP = 512
SEQ = 2048
TOK_B = 128
CAP = 32
TOKENS_B = 4096
FF = 1024
EXPERTS = 16
GROUPS = 4
EPG = 4
TOPK = 2


def shared_directions(key):
    return jax.random.truncated_normal(jax.random.fold_in(key, 71), -3.0, 3.0, (HEADS, DK))


def coherent_rows(key, salt, lowest, highest):
    level_key, noise_key = jax.random.split(jax.random.fold_in(key, salt))
    direction = shared_directions(key)
    noise = jax.random.truncated_normal(noise_key, -3.0, 3.0, (SEQ, HEADS, DK))
    levels = jax.random.uniform(level_key, (SEQ // BLOCK, HEADS), minval=lowest, maxval=highest)
    per_position = jnp.repeat(levels, BLOCK, axis=0)
    rows = per_position[:, :, None] * direction[None, :, :] + noise
    return rows.reshape(SEQ, HEADS * DK).astype(jnp.bfloat16)


def draw_query_heads_rows(key, part):
    return coherent_rows(key, 13, 0.8, 1.2)


def draw_key_heads_rows(key, part):
    return coherent_rows(key, 12, 1.2, 1.8)


def draw_head_decay_logarithm(key, part):
    pick_key, slow_key, fast_key = jax.random.split(key, 3)
    slow_share = 0.5
    chosen = jax.random.uniform(pick_key, (HEADS,)) < slow_share
    slow_rate = jnp.log(jnp.log(10.0) / (2.4 * SEQ)) + jax.random.uniform(slow_key, (HEADS,), minval=-0.3, maxval=0.3)
    fast_rate = jnp.log(1.0 / 32.0) + jax.random.uniform(fast_key, (HEADS,), minval=-0.3, maxval=0.3)
    return jnp.where(chosen, slow_rate, fast_rate).astype(jnp.float32)


def draw_decay_preactivation(key, part):
    jitter_key, device_key, block_key, run_key = jax.random.split(key, 4)
    segments_count = SEQ // TOK_AEP
    jitter = 0.5 * jax.random.truncated_normal(jitter_key, -3.0, 3.0, (HEADS, SEQ))
    per_device = jax.random.uniform(device_key, (segments_count,), minval=-1.5, maxval=1.5)
    run_start = jax.random.randint(run_key, (), 0, max(segments_count - 2, 1))
    segment_index = jnp.arange(segments_count, dtype=jnp.int32)
    in_run = (segment_index >= run_start) & (segment_index < run_start + 3)
    per_device = jnp.where(in_run, -3.0, per_device)
    per_block = jax.random.uniform(block_key, (SEQ // BLOCK,), minval=-0.5, maxval=0.5)
    offsets = jnp.repeat(per_device, TOK_AEP) + jnp.repeat(per_block, BLOCK)
    return jnp.clip(jitter + offsets[None, :], -5.0, 5.0).astype(jnp.bfloat16)


def draw_extra_log_decay(key, part):
    place_key, depth_key = jax.random.split(key)
    half_length = SEQ // 2
    places = jax.random.randint(place_key, (HEADS, 2), 0, half_length) + jnp.array([0, half_length], jnp.int32)[None, :]
    depths = jnp.log(jax.random.uniform(depth_key, (HEADS, 2), minval=0.5, maxval=0.8))
    positions = jnp.arange(SEQ, dtype=jnp.int32)
    markers = (positions[None, None, :] == places[:, :, None]).astype(jnp.float32)
    return jnp.sum(markers * depths[:, :, None], axis=1).astype(jnp.float32)


def route_block(block_key):
    hot_key, split_key, order_key = jax.random.split(block_key, 3)
    hot_rows = EPG * CAP // 2
    hot_group = jax.random.randint(hot_key, (), 0, GROUPS)
    remain = jnp.asarray(TOK_B - hot_rows, jnp.int32)
    split_keys = jax.random.split(split_key, GROUPS - 1)
    others = []
    for number in range(GROUPS - 2):
        lowest = jnp.maximum(0, remain - hot_rows * (GROUPS - 2 - number))
        highest = jnp.minimum(hot_rows, remain)
        counted = jax.random.randint(split_keys[number], (), lowest, highest + 1).astype(jnp.int32)
        others.append(counted)
        remain = remain - counted
    others.append(remain)
    other_counts = jnp.stack(others).astype(jnp.int32)
    group_index = jnp.arange(GROUPS, dtype=jnp.int32)
    shifted = jnp.clip(group_index - (group_index > hot_group).astype(jnp.int32), 0, GROUPS - 2)
    counts = jnp.where(group_index == hot_group, hot_rows, other_counts[shifted]).astype(jnp.int32)
    group_ends = jnp.cumsum(counts)
    starts = group_ends - counts
    places = jax.random.permutation(order_key, TOK_B).astype(jnp.int32)
    groups = jnp.sum((places[:, None] >= group_ends[None, :]).astype(jnp.int32), axis=1)
    within = places - starts[groups]
    first_id = groups * EPG + within % EPG
    second = groups * EPG + (within + 1 + within // EPG % (EPG - 1)) % EPG
    return jnp.stack([first_id, second], axis=1).astype(jnp.int32)


def draw_expert_choice_index(key, part):
    block_keys = jax.random.split(key, TOKENS_B // TOK_B)
    return jax.vmap(route_block)(block_keys).reshape(TOKENS_B, TOPK).astype(jnp.int32)


def shard_levels(rng, shape, cuts, smallest, top_value):
    loudness, own = 1.0, jax.random.fold_in(rng, 6)
    for dim, blocks in cuts:
        draws = jnp.exp(jax.random.uniform(jax.random.fold_in(own, dim), (blocks,), jnp.float32, smallest / len(cuts), top_value / len(cuts)))
        loudness = loudness * jnp.repeat(draws, shape[dim] // blocks).reshape([-1 if axis == dim else 1 for axis in range(len(shape))])
    return loudness


def normal_values(own_key, extent, deviation, bound, cuts=(), kind=jnp.bfloat16):
    factor_of = shard_levels(own_key, extent, cuts, -0.22, 0.18) if cuts else 1.0
    drawn = jax.random.normal(own_key, extent, jnp.float32) * deviation * factor_of
    return jnp.minimum(jnp.maximum(drawn, -bound), bound).astype(kind)


def setup_inputs(seed: int = 0) -> dict:
    key_of = jax.random.split(jax.random.key(seed), 17)
    query_heads_rows = draw_query_heads_rows(jax.random.fold_in(key_of[16], 71), 0)
    key_heads_rows = draw_key_heads_rows(jax.random.fold_in(key_of[16], 71), 0)
    value_heads_rows = normal_values(key_of[2], (SEQ, HEADS * DV), 1.0, 6.0, ((0, 4), (1, 8)))
    write_strength_logit = jnp.clip(-3.5 + 2.5 * jax.random.uniform(key_of[3], (HEADS, SEQ), jnp.float32) ** shard_levels(key_of[3], (HEADS, SEQ), ((0, 8), (1, 4)), -0.2, 0.2), -3.5, -1.0).astype(jnp.bfloat16)
    decay_preactivation = draw_decay_preactivation(jax.random.fold_in(key_of[16], 71), 0)
    head_decay_logarithm = draw_head_decay_logarithm(jax.random.fold_in(key_of[16], 71), 0)
    extra_log_decay = draw_extra_log_decay(jax.random.fold_in(key_of[16], 71), 0)
    output_weight = normal_values(key_of[7], (HEADS * DV, D), ((HEADS * DV) // 256) ** -0.5, 2.0, ((0, 8),))
    second_batch_tokens = normal_values(key_of[8], (TOKENS_B, D), 1.0, 6.0, ((0, 32),))
    expert_norm_scale = jnp.clip(1.0 + 0.18 * jax.random.normal(key_of[9], (D,), jnp.float32), 0.1, 1.9)
    expert_choice_index = draw_expert_choice_index(jax.random.fold_in(key_of[16], 71), 0)
    group_router_weight = jnp.clip(0.25 + 0.75 * jax.random.uniform(key_of[11], (TOKENS_B,), jnp.float32) ** shard_levels(key_of[11], (TOKENS_B,), ((0, 32),), -0.2, 0.2), 0.25, 1.0)
    expert_logit_difference = normal_values(key_of[12], (TOKENS_B,), 1.5, 8.0, ((0, 32),), jnp.float32)
    expert_gate_weight = normal_values(key_of[13], (EXPERTS, FF, D), D ** -0.5, 0.125, ((0, 4), (1, 8)))
    expert_up_weight = normal_values(key_of[14], (EXPERTS, FF, D), D ** -0.5, 0.125, ((0, 4), (1, 8)))
    expert_down_weight = normal_values(key_of[15], (EXPERTS, FF, D), (FF // 4) ** -0.5, 0.375, ((0, 4), (1, 8)))
    return dict(query_heads_rows=query_heads_rows, key_heads_rows=key_heads_rows, value_heads_rows=value_heads_rows, write_strength_logit=write_strength_logit, decay_preactivation=decay_preactivation, head_decay_logarithm=head_decay_logarithm, extra_log_decay=extra_log_decay, output_weight=output_weight, second_batch_tokens=second_batch_tokens, expert_norm_scale=expert_norm_scale, expert_choice_index=expert_choice_index, group_router_weight=group_router_weight, expert_logit_difference=expert_logit_difference, expert_gate_weight=expert_gate_weight, expert_up_weight=expert_up_weight, expert_down_weight=expert_down_weight)


precise_setting = lax.Precision.HIGHEST
norm_eps = 1e-06

def unit_rows(matrix):
    return matrix * lax.rsqrt(lax.optimization_barrier(jnp.sum(matrix * matrix, axis=-1, keepdims=True)) + norm_eps)

def block_terms(query_block, key_block, value_block, decay_logarithm, strength):
    span_len = query_block.shape[2]
    dim_value = value_block.shape[-1]
    cumulative = jnp.cumsum(decay_logarithm, axis=-1)
    within = jnp.tril(jnp.ones((span_len, span_len), bool))
    strict = jnp.tril(jnp.ones((span_len, span_len), bool), -1)
    spread = cumulative[..., :, None] - cumulative[..., None, :]
    decayed = jnp.where(within, jnp.exp(jnp.where(within, spread, 0.0)), 0.0)
    weighted = key_block * strength[..., None]
    lower_part = jnp.where(strict, jnp.einsum('hnid,hnjd->hnij', weighted, key_block, precision=precise_setting) * decayed, 0.0)
    system = lower_part + jnp.eye(span_len, dtype=jnp.float32)
    rhs_cols = jnp.concatenate([value_block * strength[..., None], weighted * jnp.exp(cumulative)[..., None]], axis=-1)
    solved = jax.scipy.linalg.solve_triangular(system, rhs_cols, lower=True, unit_diagonal=True)
    updated_values = solved[..., :dim_value]
    delta_corrections = solved[..., dim_value:]
    scores = jnp.where(within, jnp.einsum('hnid,hnjd->hnij', query_block, key_block, precision=precise_setting) * decayed, 0.0)
    decayed_queries = query_block * jnp.exp(cumulative)[..., None]
    decayed_keys = key_block * jnp.exp(cumulative[..., -1:] - cumulative)[..., None]
    block_retention = jnp.exp(cumulative[..., -1])
    return (decayed_queries, decayed_keys, updated_values, delta_corrections, scores, block_retention)

def carry_step(recurrent_state, inputs):
    decayed_queries, decayed_keys, updated_values, delta_corrections, scores, block_retention = inputs
    value_updates = updated_values - jnp.einsum('jdb,jbu->jdu', delta_corrections, recurrent_state, precision=precise_setting)
    final_output = jnp.einsum('jdb,jbu->jdu', decayed_queries, recurrent_state, precision=precise_setting)
    final_output = final_output + jnp.einsum('hcj,hjv->hcv', scores, value_updates, precision=precise_setting)
    recurrent_state = recurrent_state * block_retention[:, None, None] + jnp.einsum('rpq,rpd->rqd', decayed_keys, value_updates, precision=precise_setting)
    return (recurrent_state, final_output)

def mixer_portion(query_heads_rows, key_heads_rows, value_heads_rows, write_strength_logit, decay_preactivation, head_decay_logarithm, extra_log_decay, output_weight):
    length = query_heads_rows.shape[0]
    blocks = length // BLOCK

    def heads_first(matrix):
        spread_out = matrix.astype(jnp.float32).reshape(length, HEADS, -1).transpose(1, 0, 2)
        return spread_out.reshape(HEADS, blocks, BLOCK, -1)
    query_block = unit_rows(heads_first(query_heads_rows)) * DK ** (-0.5)
    key_block = unit_rows(heads_first(key_heads_rows))
    value_block = heads_first(value_heads_rows)
    strength = jax.nn.sigmoid(write_strength_logit.astype(jnp.float32)).reshape(HEADS, blocks, BLOCK)
    decay_logarithm = -jnp.exp(head_decay_logarithm)[:, None] * jax.nn.softplus(decay_preactivation.astype(jnp.float32)) + extra_log_decay
    decay_logarithm = decay_logarithm.reshape(HEADS, blocks, BLOCK)
    terms = block_terms(query_block, key_block, value_block, decay_logarithm, strength)
    inputs = tuple((jnp.moveaxis(term, 1, 0) for term in terms))
    _, outputs = lax.scan(carry_step, jnp.zeros((HEADS, DK, DV), jnp.float32), inputs)
    attention_result = outputs.transpose(0, 2, 1, 3).reshape(length, HEADS * DV).astype(jnp.bfloat16)
    return jnp.dot(attention_result.astype(jnp.float32), output_weight.astype(jnp.float32), preferred_element_type=jnp.float32).astype(jnp.bfloat16)

def experts_part(second_batch_tokens, expert_norm_scale, expert_choice_index, group_router_weight, expert_logit_difference, expert_gate_weight, expert_up_weight, expert_down_weight):
    widened = second_batch_tokens.astype(jnp.float32)
    normed = (widened * lax.rsqrt(lax.optimization_barrier(jnp.mean(widened * widened, axis=-1, keepdims=True)) + norm_eps) * expert_norm_scale).astype(jnp.bfloat16)
    token_count = second_batch_tokens.shape[0]
    width_model = second_batch_tokens.shape[1]
    flat_ids = expert_choice_index.reshape(-1).astype(jnp.int32)
    copy_count = flat_ids.shape[0]
    sorted_order = jnp.argsort(flat_ids, stable=True).astype(jnp.int32)
    sorted_ids = flat_ids[sorted_order]
    counts = lax.optimization_barrier(jnp.sum((flat_ids[:, None] == jnp.arange(EXPERTS, dtype=jnp.int32)[None, :]).astype(jnp.int32), axis=0))
    starts = jnp.cumsum(counts) - counts
    padded = (counts + 127) // 128 * 128
    pad_ends = jnp.cumsum(padded)
    pad_starts = pad_ends - padded
    destination = (pad_starts[sorted_ids] + jnp.arange(copy_count, dtype=jnp.int32) - starts[sorted_ids]).astype(jnp.int32)
    segments = -(-copy_count // 128) + EXPERTS
    source = jnp.full((segments * 128,), token_count, jnp.int32).at[destination].set((sorted_order // TOPK).astype(jnp.int32))
    padded_rows = jnp.concatenate([normed, jnp.zeros((1, width_model), jnp.bfloat16)], axis=0)
    gathered = padded_rows[source]
    seg_expert = jnp.minimum(jnp.searchsorted(pad_ends, jnp.arange(segments, dtype=jnp.int32) * 128, side='right'), EXPERTS - 1).astype(jnp.int32)

    def one_segment(operands):
        segment_rows, expert = operands
        gating = jnp.dot(segment_rows.astype(jnp.float32), expert_gate_weight[expert].T.astype(jnp.float32), preferred_element_type=jnp.float32)
        upward = jnp.dot(segment_rows.astype(jnp.float32), expert_up_weight[expert].T.astype(jnp.float32), preferred_element_type=jnp.float32)
        hidden = (jax.nn.silu(gating) * upward).astype(jnp.bfloat16)
        return jnp.dot(hidden.astype(jnp.float32), expert_down_weight[expert].astype(jnp.float32), preferred_element_type=jnp.float32).astype(jnp.bfloat16)
    results = lax.map(one_segment, (gathered.reshape(segments, 128, width_model), seg_expert))
    per_copy = results.reshape(-1, width_model)[destination]
    unsorted = jnp.zeros((copy_count, width_model), jnp.bfloat16).at[sorted_order].set(per_copy)
    copies = unsorted.reshape(token_count, TOPK, width_model).astype(jnp.float32)
    leading = jax.nn.sigmoid(expert_logit_difference)
    weights = group_router_weight[:, None] * jnp.stack([leading, 1.0 - leading], axis=-1)
    return lax.optimization_barrier(jnp.sum(weights[..., None] * copies, axis=1)).astype(jnp.bfloat16)

def reference(query_heads_rows, key_heads_rows, value_heads_rows, write_strength_logit, decay_preactivation, head_decay_logarithm, extra_log_decay, output_weight, second_batch_tokens, expert_norm_scale, expert_choice_index, group_router_weight, expert_logit_difference, expert_gate_weight, expert_up_weight, expert_down_weight):
    mixer_output_first = mixer_portion(query_heads_rows, key_heads_rows, value_heads_rows, write_strength_logit, decay_preactivation, head_decay_logarithm, extra_log_decay, output_weight)
    expert_out = experts_part(second_batch_tokens, expert_norm_scale, expert_choice_index, group_router_weight, expert_logit_difference, expert_gate_weight, expert_up_weight, expert_down_weight)
    return (mixer_output_first, expert_out)
```

```python
import functools

import jax
import jax.numpy as jnp
from jax import lax
from jax.experimental import pallas as pl
from jax.experimental.pallas import tpu as pltpu
from jax.sharding import PartitionSpec as P

DK = 128
DV = 128
CAP = 32
EXPERTS = 16
EPG = 4
TOPK = 2
CORES = 2
META = 128
CHUNK = 128
NORM_EPS = 1e-06


F32 = jnp.float32
BF16 = jnp.bfloat16
EXACT = lax.Precision.HIGHEST
VMEM = pl.BlockSpec(memory_space=pltpu.VMEM)
SMEM = pl.BlockSpec(memory_space=pltpu.SMEM)


def cost(flops, moved):
    return pl.CostEstimate(flops=int(flops), bytes_accessed=int(moved), transcendentals=0)


def mm(a, b):
    return jnp.dot(a, b, precision=EXACT, preferred_element_type=F32)


def mixer_kernel(q_ref, k_ref, v_ref, row_ref, col_ref, local_ref, proj_ref, state_ref, map_ref):
    length = q_ref.shape[0]
    chunks = length // CHUNK
    i = lax.broadcasted_iota(jnp.int32, (CHUNK, CHUNK), 0)
    j = lax.broadcasted_iota(jnp.int32, (CHUNK, CHUNK), 1)
    every = range(chunks)

    def unit(ref, c):
        x = ref[c * CHUNK : (c + 1) * CHUNK, :].astype(F32)
        return x * lax.rsqrt(jnp.sum(x * x, axis=-1, keepdims=True) + NORM_EPS)

    q = [unit(q_ref, c) * DK**-0.5 for c in every]
    k = [unit(k_ref, c) for c in every]
    kt = [jnp.transpose(x) for x in k]
    v = [v_ref[c * CHUNK : (c + 1) * CHUNK, :].astype(F32) for c in every]
    row = [row_ref[0, c : c + 1, :] for c in every]
    col = [col_ref[0, :, c : c + 1] for c in every]
    beta = [col_ref[0, :, chunks + c : chunks + c + 1] for c in every]
    last = [r[:, CHUNK - 1 :] for r in row]
    decay = [jnp.where(i >= j, jnp.exp(jnp.where(i >= j, col[c] - row[c], 0.0)), 0.0) for c in every]
    gram = [mm(k[c], kt[c]) for c in every]
    lower = [jnp.where(i > j, gram[c] * decay[c] * beta[c], 0.0) for c in every]
    scores = [mm(q[c], kt[c]) * decay[c] for c in every]
    eye = jnp.where(i == j, 1.0, 0.0)
    small = 16
    near = (i // small) == (j // small)
    power = [jnp.where(near, x, 0.0) for x in lower]
    inverse = [eye - x for x in power]
    reach = 2
    while reach < small:
        power = [mm(x, x) for x in power]
        inverse = [x + mm(x, y) for x, y in zip(inverse, power)]
        reach *= 2
    while small < CHUNK:
        band = ((i // (2 * small)) == (j // (2 * small))) & ((i // small) != (j // small))
        half = [mm(jnp.where(band, x, 0.0), y) for x, y in zip(lower, inverse)]
        inverse = [y - mm(y, x) for x, y in zip(half, inverse)]
        small *= 2
    grown = [jnp.exp(col[c]) for c in every]
    rhs = [jnp.concatenate([v[c] * beta[c], k[c] * (beta[c] * grown[c])], axis=1) for c in every]
    solved = [mm(inverse[c], rhs[c]) for c in every]
    blank = jnp.zeros((CHUNK, DK), F32)
    joint = jnp.concatenate([jnp.zeros((DK, DV), F32), eye], axis=1)
    for c in every:
        update = jnp.concatenate([solved[c][:, :DV], blank], axis=1) - mm(solved[c][:, DV:], joint)
        out = mm(q[c] * grown[c], joint) + mm(scores[c], update)
        joint = joint * jnp.exp(last[c]) + mm(kt[c] * jnp.exp(last[c] - row[c]), update)
        local_ref[c * CHUNK : (c + 1) * CHUNK, :] = out[:, :DV]
        proj_ref[c * CHUNK : (c + 1) * CHUNK, :] = out[:, DV:]
    state_ref[0] = joint[:, :DV]
    map_ref[0] = joint[:, DV:]


def mixer_local(queries, keys, values, rows, cols):
    length, width = queries.shape
    heads = width // DK
    chunks = length // CHUNK
    tall = pl.BlockSpec((length, DK), lambda h: (0, h))
    square = pl.BlockSpec((1, DK, DV), lambda h: (h, 0, 0))
    return pl.pallas_call(
        mixer_kernel,
        grid=(heads,),
        in_specs=[
            tall,
            tall,
            tall,
            pl.BlockSpec((1, chunks, CHUNK), lambda h: (h, 0, 0)),
            pl.BlockSpec((1, CHUNK, 2 * chunks), lambda h: (h, 0, 0)),
        ],
        out_specs=[tall, tall, square, square],
        out_shape=[
            jax.ShapeDtypeStruct((length, width), F32),
            jax.ShapeDtypeStruct((length, width), F32),
            jax.ShapeDtypeStruct((heads, DK, DV), F32),
            jax.ShapeDtypeStruct((heads, DK, DV), F32),
        ],
        cost_estimate=cost(heads * chunks * 26 * 6 * 2 * 128**3, length * width * 14),
        name="mixer_local",
    )(queries, keys, values, rows, cols)


def attend_kernel(local_ref, proj_ref, state_ref, out_ref):
    out_ref[...] = (local_ref[...] + mm(proj_ref[...], state_ref[0])).astype(BF16)


def attend(local, proj, state):
    length, width = local.shape
    heads = width // DV
    tall = pl.BlockSpec((length, DV), lambda h: (0, h))
    return pl.pallas_call(
        attend_kernel,
        grid=(heads,),
        in_specs=[tall, tall, pl.BlockSpec((1, DK, DV), lambda h: (h, 0, 0))],
        out_specs=tall,
        out_shape=jax.ShapeDtypeStruct((length, width), BF16),
        cost_estimate=cost(6 * 2 * length * width * DK, length * width * 10),
        name="attend",
    )(local, proj, state)


def prepare_kernel(own, x_ref, scale_ref, index_ref, weight_ref, logit_ref, out_ref):
    rows, width = x_ref.shape
    x = x_ref[...].astype(F32)
    inv = lax.rsqrt(jnp.mean(x * x, axis=-1, keepdims=True) + NORM_EPS)
    out_ref[:, :width] = (x * inv * scale_ref[...]).astype(BF16)
    shift = own.bit_length() - 1
    first, second = index_ref[:, 0:1], index_ref[:, 1:2]
    home = [lax.shift_right_logical(x, jnp.full_like(x, shift)) for x in (first, second)]
    place = [x & (own - 1) for x in (first, second)]
    lane = lax.broadcasted_iota(jnp.int32, (rows, META), 1)
    member = jnp.where((lane == home[0]) | (lane == home[1]), 1.0, 0.0).astype(BF16)
    ti = lax.broadcasted_iota(jnp.int32, (rows, rows), 0)
    tj = lax.broadcasted_iota(jnp.int32, (rows, rows), 1)
    before = jnp.where(ti > tj, 1.0, 0.0).astype(BF16)
    count = jnp.dot(before, member, preferred_element_type=F32)
    rank = [jnp.sum(jnp.where(lane == x, count, 0.0), axis=1, keepdims=True) for x in home]
    lead = jax.nn.sigmoid(logit_ref[...])
    mixing = [weight_ref[...] * lead, weight_ref[...] * (1.0 - lead)]
    high = [x.astype(BF16).astype(F32) for x in mixing]
    low = [x - y for x, y in zip(mixing, high)]
    columns = [x.astype(F32) for x in home] + rank + [x.astype(F32) for x in place] + high + low
    meta = jnp.zeros((rows, META), F32)
    for number, column in enumerate(columns):
        meta = jnp.where(lane == number, column, meta)
    out_ref[:, width:] = meta.astype(BF16)


def prepare(own, tokens, scale, index, weight, logit):
    rows, width = tokens.shape
    return pl.pallas_call(
        functools.partial(prepare_kernel, own),
        in_specs=[VMEM] * 5,
        out_specs=VMEM,
        out_shape=jax.ShapeDtypeStruct((rows, width + META), BF16),
        cost_estimate=cost(rows * width * 8, rows * width * 4),
        name="prepare",
    )(tokens, scale.reshape(1, -1), index, weight.reshape(-1, 1), logit.reshape(-1, 1))


def placement(me, meta, total, slots):
    rows = meta.shape[0]
    lane = lax.broadcasted_iota(jnp.int32, (rows, total), 1)
    home = [meta[:, x : x + 1].astype(jnp.int32) for x in (0, 1)]
    rank = [meta[:, x : x + 1].astype(jnp.int32) for x in (2, 3)]
    spot = [(x ^ me) * slots + y for x, y in zip(home, rank)]
    return jnp.where((lane == spot[0]) | (lane == spot[1]), 1.0, 0.0)


def dispatch_kernel(peers, slots, me_ref, block_ref, *out_refs):
    width = block_ref.shape[1] - META
    meta = block_ref[:, width:].astype(F32)
    pick = jnp.transpose(placement(me_ref[0], meta, peers * slots, slots)).astype(BF16)
    for number, out_ref in enumerate(out_refs):
        part = pick[number * slots : (number + 1) * slots, :]
        out_ref[...] = jnp.dot(part, block_ref[...], preferred_element_type=F32).astype(BF16)


def dispatch(peers, slots, me, block):
    rows, width = block.shape
    return pl.pallas_call(
        functools.partial(dispatch_kernel, peers, slots),
        in_specs=[SMEM, VMEM],
        out_specs=[VMEM] * peers,
        out_shape=[jax.ShapeDtypeStruct((slots, width), BF16)] * peers,
        cost_estimate=cost(2 * peers * slots * rows * width, (rows + peers * slots) * width * 2),
        name="dispatch",
    )(me, block)


def expert_kernel(peers, slots, me_ref, *refs):
    x_refs, refs = refs[:peers], refs[peers:]
    gate_a, gate_b, up_a, up_b, down_a, down_b = refs[:6]
    out_refs, (x_all, total) = refs[6 : 6 + peers], refs[6 + peers :]
    expert = pl.program_id(0)
    width = total.shape[1]
    units = 2 * gate_a.shape[1]

    @pl.when(expert == 0)
    def _():
        for number, x_ref in enumerate(x_refs):
            x_all[number * slots : (number + 1) * slots, :] = x_ref[...]

    meta = x_all[:, width:].astype(F32)
    me = me_ref[0].astype(F32)
    here = expert.astype(F32)
    weight = jnp.zeros((peers * slots, 1), F32)
    for choice in range(TOPK):
        fits = (meta[:, choice : choice + 1] == me) & (meta[:, 4 + choice : 5 + choice] == here)
        value = meta[:, 6 + choice : 7 + choice] + meta[:, 8 + choice : 9 + choice]
        weight = weight + jnp.where(fits, value, 0.0)
    inner = jnp.concatenate([gate_a[0], gate_b[0], up_a[0], up_b[0]], axis=0)
    both = lax.dot_general(
        x_all[:, :width], inner, (((1,), (1,)), ((), ())), preferred_element_type=F32
    )
    gating, upward = both[:, :units], both[:, units:]
    hidden = (gating / (1.0 + jnp.exp(-gating)) * upward * weight).astype(BF16)
    down = jnp.concatenate([down_a[0], down_b[0]], axis=0)
    part = jnp.dot(hidden, down, preferred_element_type=F32)

    @pl.when(expert == 0)
    def _():
        total[...] = part

    @pl.when(expert > 0)
    def _():
        total[...] += part

    @pl.when(expert == pl.num_programs(0) - 1)
    def _():
        for number, out_ref in enumerate(out_refs):
            out_ref[...] = total[number * slots : (number + 1) * slots, :].astype(BF16)


def expert_part(peers, slots, me, arrived, weights):
    own, units, width = weights[0].shape
    rows = peers * slots
    piece = pl.BlockSpec((1, units, width), lambda x: (x, 0, 0))
    whole = pl.BlockSpec((slots, width + META), lambda x: (0, 0))
    return pl.pallas_call(
        functools.partial(expert_kernel, peers, slots),
        grid=(own,),
        in_specs=[SMEM] + [whole] * peers + [piece] * 6,
        out_specs=[pl.BlockSpec((slots, width), lambda x: (0, 0))] * peers,
        out_shape=[jax.ShapeDtypeStruct((slots, width), BF16)] * peers,
        scratch_shapes=[pltpu.VMEM((rows, width + META), BF16), pltpu.VMEM((rows, width), F32)],
        cost_estimate=cost(12 * own * units * rows * width, 12 * own * units * width + 4 * rows * width),
        name="expert_part",
    )(me, *arrived, *weights)


def collect_kernel(peers, slots, me_ref, meta_ref, *refs):
    pick = placement(me_ref[0], meta_ref[...].astype(F32), peers * slots, slots).astype(BF16)
    back = jnp.concatenate([x[...] for x in refs[:peers]], axis=0)
    found = jnp.dot(pick, back, preferred_element_type=F32)
    for extra in refs[peers:-1]:
        found = found + extra[...].astype(F32)
    refs[-1][...] = found.astype(BF16)


def collect(peers, slots, me, block, returned, extra):
    rows = block.shape[0]
    width = block.shape[1] - META
    full = lambda shape: pl.BlockSpec(shape, lambda x: (0, 0))
    return pl.pallas_call(
        functools.partial(collect_kernel, peers, slots),
        grid=(1,),
        in_specs=[SMEM, pl.BlockSpec((rows, META), lambda x: (0, width // META))]
        + [full((slots, width))] * peers
        + [full((rows, width))] * len(extra),
        out_specs=full((rows, width)),
        out_shape=jax.ShapeDtypeStruct((rows, width), BF16),
        cost_estimate=cost(2 * rows * peers * slots * width, (2 * rows + peers * slots) * width * 2),
        name="collect",
    )(me, block, *returned, *extra)


def shards(
    query_heads_rows,
    key_heads_rows,
    value_heads_rows,
    write_strength_logit,
    decay_preactivation,
    head_decay_logarithm,
    extra_log_decay,
    output_weight,
    second_batch_tokens,
    expert_norm_scale,
    expert_choice_index,
    group_router_weight,
    expert_logit_difference,
    expert_gate_weight,
    expert_up_weight,
    expert_down_weight,
):
    ep, tp = lax.axis_size("ep"), lax.axis_size("tp")
    depth = tp // CORES
    me = lax.axis_index("ep")
    rank = lax.axis_index("tp")
    level, core = rank // CORES, rank % CORES
    pair = [(x, x ^ 1) for x in range(tp)]
    ring = [(x, (x + CORES) % tp) for x in range(tp)]

    def swap(x):
        return lax.ppermute(x, "tp", pair)

    def step_on(x):
        return lax.ppermute(x, "tp", ring)

    def trade(x, distance):
        return lax.ppermute(x, "ep", [(y, y ^ distance) for y in range(ep)])

    me1 = me.astype(jnp.int32).reshape(1)
    own = EXPERTS // ep
    tokens = second_batch_tokens.shape[0]
    slots = own * CAP // TOPK if own % EPG == 0 else min(own * CAP, tokens)

    block = prepare(
        own,
        second_batch_tokens,
        expert_norm_scale,
        expert_choice_index,
        group_router_weight,
        expert_logit_difference,
    )
    weights = []
    for shard in (expert_gate_weight, expert_up_weight, expert_down_weight):
        weights += [shard, swap(shard)]
    blocks, backs = [], []
    for hop in range(depth):
        blocks.append(block)
        sent = dispatch(ep, slots, me1, block)
        if hop < depth - 1:
            block = step_on(block)
        arrived = [sent[0]] + [trade(sent[x], x) for x in range(1, ep)]
        produced = expert_part(ep, slots, me1, arrived, weights)
        backs.append([produced[0]] + [trade(produced[x], x) for x in range(1, ep)])
    running = []
    for hop in range(1, depth):
        running = [step_on(collect(ep, slots, me1, blocks[hop], backs[hop], running))]
    expert_out = collect(ep, slots, me1, blocks[0], backs[0], running)

    length = query_heads_rows.shape[0]
    heads = head_decay_logarithm.shape[0]
    chunks = length // CHUNK
    strength = jax.nn.sigmoid(write_strength_logit.astype(F32)).reshape(heads, chunks, CHUNK)
    log_decay = (
        -jnp.exp(head_decay_logarithm)[:, None]
        * jax.nn.softplus(decay_preactivation.astype(F32))
        + extra_log_decay
    ).reshape(heads, chunks, CHUNK)
    upto = jnp.triu(jnp.ones((CHUNK, CHUNK), F32))
    summed = jnp.einsum("hcj,ji->hci", log_decay, upto, precision=EXACT)
    cols = jnp.concatenate([summed, strength], axis=1).transpose(0, 2, 1)
    local, proj, state, transfer = mixer_local(
        query_heads_rows, key_heads_rows, value_heads_rows, summed, cols
    )
    onward = state
    line = [(x, x + 1) for x in range(ep - 1)]
    for hop in range(ep - 1):
        incoming = lax.ppermute(onward, "ep", line)
        if hop < ep - 2:
            onward = state + jnp.einsum("hij,hjv->hiv", transfer, incoming, precision=EXACT)
    attention = attend(local, proj, incoming).reshape(depth, CORES, length // tp, heads * DV)
    mine = lax.dynamic_index_in_dim(attention, core, 1, keepdims=False)
    theirs = swap(lax.dynamic_index_in_dim(attention, 1 - core, 1, keepdims=False))
    both = jnp.concatenate([mine, theirs], axis=-1)
    out_weight = jnp.concatenate([output_weight, swap(output_weight)], axis=0)
    partial = jnp.einsum("zrf,fd->zrd", both, out_weight, preferred_element_type=F32).astype(BF16)

    def piece(hop):
        at = (level + depth - hop) % depth
        return lax.dynamic_index_in_dim(partial, at, 0, keepdims=False).astype(F32)

    moving = None
    for hop in range(1, depth):
        part = piece(hop)
        if moving is not None:
            part = part + moving.astype(F32)
        moving = step_on(part.astype(BF16))
    mixed = piece(0)
    if moving is not None:
        mixed = mixed + moving.astype(F32)
    return (mixed.astype(BF16), expert_out)


def solution(mesh):
    in_specs = (
        P("ep", "tp"),
        P("ep", "tp"),
        P("ep", "tp"),
        P("tp", "ep"),
        P("tp", "ep"),
        P("tp"),
        P("tp", "ep"),
        P("tp", None),
        P(("ep", "tp"), None),
        P(),
        P(("ep", "tp"), None),
        P(("ep", "tp")),
        P(("ep", "tp")),
        P("ep", "tp", None),
        P("ep", "tp", None),
        P("ep", "tp", None),
    )
    out_specs = (P(("ep", "tp"), None), P(("ep", "tp"), None))
    return jax.shard_map(shards, mesh=mesh, in_specs=in_specs, out_specs=out_specs, check_vma=False)
```

```python
import functools

import jax
import jax.numpy as jnp
from jax import lax
from jax.experimental import pallas as pl
from jax.experimental.pallas import tpu as pltpu
from jax.sharding import PartitionSpec as P


DK = 128
DV = 128
CAP = 32
EXPERTS = 16
EPG = 4
TOPK = 2
CORES = 2
META = 128
CHUNK = 128
NORM_EPS = 1e-06


F32 = jnp.float32
BF16 = jnp.bfloat16
EXACT = lax.Precision.HIGHEST
VMEM = pl.BlockSpec(memory_space=pltpu.VMEM)
HBM = pl.BlockSpec(memory_space=pltpu.HBM)
SMEM = pl.BlockSpec(memory_space=pltpu.SMEM)


def room(mib):
    return pltpu.CompilerParams(vmem_limit_bytes=mib * 2**20)


def cost(flops, moved):
    return pl.CostEstimate(flops=int(flops), bytes_accessed=int(moved), transcendentals=0)


def mm(a, b):
    return jnp.dot(a, b, precision=EXACT, preferred_element_type=F32)


def mixer_kernel(head, rate_ref, q_ref, k_ref, v_ref, write_ref, decay_ref, extra_ref, local_ref, proj_ref, joint_ref):
    length = q_ref.shape[0]
    chunks = length // CHUNK
    i = lax.broadcasted_iota(jnp.int32, (CHUNK, CHUNK), 0)
    j = lax.broadcasted_iota(jnp.int32, (CHUNK, CHUNK), 1)
    every = range(chunks)
    spans = [slice(c * CHUNK, (c + 1) * CHUNK) for c in every]

    def unit(ref, n):
        x = ref[spans[n], :].astype(F32)
        return x * lax.rsqrt(jnp.sum(x * x, axis=-1, keepdims=True) + NORM_EPS)

    q = [unit(q_ref, n) * DK**-0.5 for n in every]
    k = [unit(k_ref, n) for n in every]
    kt = [jnp.transpose(x) for x in k]
    v = [v_ref[spans[n], :].astype(F32) for n in every]
    raised = decay_ref[head : head + 1, :].astype(F32)
    soft = jnp.maximum(raised, 0.0) + jnp.log(1.0 + jnp.exp(-jnp.abs(raised)))
    rate = jnp.exp(jnp.full((1, length), rate_ref[head], F32))
    drops = extra_ref[head : head + 1, :] - rate * soft
    writes = jax.nn.sigmoid(write_ref[head : head + 1, :].astype(F32))
    drops = jnp.concatenate([drops[:, x] for x in spans], axis=0)
    writes = jnp.concatenate([writes[:, x] for x in spans], axis=0)
    summed = mm(drops, jnp.where(i <= j, 1.0, 0.0))
    columns = jnp.transpose(jnp.concatenate([summed, writes], axis=0))
    row = [summed[n : n + 1, :] for n in every]
    col = [columns[:, n : n + 1] for n in every]
    beta = [columns[:, len(every) + n : len(every) + n + 1] for n in every]
    last = [r[:, CHUNK - 1 :] for r in row]
    decay = [jnp.where(i >= j, jnp.exp(jnp.where(i >= j, col[n] - row[n], 0.0)), 0.0) for n in every]
    gram = [mm(k[n], kt[n]) for n in every]
    lower = [jnp.where(i > j, gram[n] * decay[n] * beta[n], 0.0) for n in every]
    scores = [mm(q[n], kt[n]) * decay[n] for n in every]
    eye = jnp.where(i == j, 1.0, 0.0)
    small = 16
    near = (i // small) == (j // small)
    power = [jnp.where(near, x, 0.0) for x in lower]
    inverse = [eye - x for x in power]
    reach = 2
    while reach < small:
        power = [mm(x, x) for x in power]
        inverse = [x + mm(x, y) for x, y in zip(inverse, power)]
        reach *= 2
    while small < CHUNK:
        band = ((i // (2 * small)) == (j // (2 * small))) & ((i // small) != (j // small))
        half = [mm(jnp.where(band, x, 0.0), y) for x, y in zip(lower, inverse)]
        inverse = [y - mm(y, x) for x, y in zip(half, inverse)]
        small *= 2
    grown = [jnp.exp(x) for x in col]
    rhs = [jnp.concatenate([v[n] * beta[n], k[n] * (beta[n] * grown[n])], axis=1) for n in every]
    solved = [mm(inverse[n], rhs[n]) for n in every]
    blank = jnp.zeros((CHUNK, DK), F32)
    start = jnp.concatenate([jnp.zeros((DK, DV), F32), eye], axis=1)
    joint = start
    for n in every:
        update = jnp.concatenate([solved[n][:, :DV], blank], axis=1) - mm(solved[n][:, DV:], joint)
        out = mm(q[n] * grown[n], joint) + mm(scores[n], update)
        joint = joint * jnp.exp(last[n]) + mm(kt[n] * jnp.exp(last[n] - row[n]), update)
        local_ref[spans[n], :] = out[:, :DV]
        proj_ref[spans[n], :] = out[:, DV:]
    joint_ref[...] = joint


def mixer_local(head, rates, queries, keys, values, write, decay, extra):
    length = queries.shape[0]
    tall = pl.BlockSpec((length, DK), lambda x: (0, head))
    gate = pl.BlockSpec(write.shape, lambda x: (0, 0))
    flat = pl.BlockSpec((length, DK), lambda x: (0, 0))
    return pl.pallas_call(
        functools.partial(mixer_kernel, head),
        grid=(1,),
        in_specs=[SMEM] + [tall] * 3 + [gate] * 3,
        out_specs=[flat, flat, pl.BlockSpec((DK, DV + DK), lambda x: (0, 0))],
        out_shape=[
            jax.ShapeDtypeStruct((length, DV), F32),
            jax.ShapeDtypeStruct((length, DK), F32),
            jax.ShapeDtypeStruct((DK, DV + DK), F32),
        ],
        cost_estimate=cost(length // CHUNK * 26 * 6 * 2 * 128**3, length * DK * 14),
        name="mixer_local",
    )(rates, queries, keys, values, write, decay, extra)


def join_kernel(late_ref, own_ref, got_ref, inner_ref, own_out, inner_out):
    late = late_ref[0] > 0
    for h in range(own_ref.shape[0]):
        own, got, inner = own_ref[h], got_ref[h], inner_ref[h]
        first, second = jnp.where(late, got, own), jnp.where(late, own, got)
        blank = jnp.zeros_like(own[:, DV:])
        keep = lambda x: jnp.concatenate([x[:, :DV], blank], axis=1)
        own_out[h] = mm(second[:, DV:], first) + keep(second)
        inner_out[h] = jnp.where(late, mm(inner[:, DV:], got) + keep(inner), inner)


def join(late, own, got, inner):
    shape = jax.ShapeDtypeStruct(own.shape, F32)
    return pl.pallas_call(
        join_kernel,
        in_specs=[SMEM] + [VMEM] * 3,
        out_specs=[VMEM] * 2,
        out_shape=[shape, shape],
        compiler_params=room(8),
        cost_estimate=cost(own.size * 24 * DK, own.size * 20),
        name="join",
    )(late, own, got, inner)


def attend_kernel(heads, late_ref, core_ref, *refs):
    local_refs, proj_refs = refs[:heads], refs[heads : 2 * heads]
    got_ref, inner_ref, mine_ref, other_ref = refs[2 * heads :]
    late = late_ref[0] > 0
    states = []
    for h in range(heads):
        inner = inner_ref[h]
        state = mm(inner[:, DV:], got_ref[h]) + inner[:, :DV]
        states.append(jnp.where(late, state, inner[:, :DV]))
    depth, rows = mine_ref.shape[0], mine_ref.shape[1]
    for out_ref, shift in ((mine_ref, core_ref[0]), (other_ref, 1 - core_ref[0])):
        for z in range(depth):
            span = pl.ds(pl.multiple_of((z * CORES + shift) * rows, rows), rows)
            for h in range(heads):
                out = local_refs[h][span, :] + mm(proj_refs[h][span, :], states[h])
                out_ref[z, :, h * DV : (h + 1) * DV] = out.astype(BF16)


def attend(depth, late, core, local, proj, got, inner):
    heads = len(local)
    length, width = local[0].shape
    half = jax.ShapeDtypeStruct((depth, length // depth // CORES, heads * width), BF16)
    full = lambda *shape: pl.BlockSpec(shape, lambda x: (0,) * len(shape))
    return pl.pallas_call(
        functools.partial(attend_kernel, heads),
        grid=(1,),
        in_specs=[SMEM] * 2 + [full(length, width)] * (2 * heads) + [full(*got.shape), full(*inner.shape)],
        out_specs=[full(*half.shape)] * 2,
        out_shape=[half, half],
        compiler_params=room(8),
        cost_estimate=cost(6 * 2 * length * width * DK * heads, length * width * 10 * heads),
        name="attend",
    )(late, core, *local, *proj, got, inner)


def project_kernel(mine_ref, theirs_ref, own_ref, pair_ref, out_ref):
    depth, rows, width = mine_ref.shape
    left = jnp.concatenate(
        [x[...].reshape(depth * rows, width) for x in (mine_ref, theirs_ref)], axis=1
    )
    tile = 512

    def body(step, carry):
        span = pl.ds(pl.multiple_of(step * tile, tile), tile)
        right = jnp.concatenate([own_ref[:, span], pair_ref[:, span]], axis=0)
        part = jnp.dot(left, right, preferred_element_type=F32).astype(BF16)
        out_ref[:, :, span] = part.reshape(depth, rows, tile)
        return carry

    lax.fori_loop(0, out_ref.shape[2] // tile, body, 0)


def project(mine, theirs, own, pair):
    depth, rows, width = mine.shape
    wide = own.shape[1]
    return pl.pallas_call(
        project_kernel,
        in_specs=[VMEM] * 4,
        out_specs=VMEM,
        out_shape=jax.ShapeDtypeStruct((depth, rows, wide), BF16),
        compiler_params=room(8),
        cost_estimate=cost(4 * depth * rows * width * wide, 4 * width * wide + 2 * depth * rows * wide),
        name="project",
    )(mine, theirs, own, pair)


def prepare_kernel(own, peers, slots, me_ref, x_ref, scale_ref, index_ref, gain_ref, block_ref, *out_refs):
    rows, width = x_ref.shape
    x = x_ref[...].astype(F32)
    inv = lax.rsqrt(jnp.mean(x * x, axis=-1, keepdims=True) + NORM_EPS)
    block_ref[:, :width] = (x * inv * scale_ref[...]).astype(BF16)
    shift = own.bit_length() - 1
    names = jnp.transpose(jnp.concatenate([index_ref[...].astype(F32), gain_ref[...]], axis=0))
    picks = [names[:, n : n + 1].astype(jnp.int32) for n in range(TOPK)]
    gain, logit = names[:, TOPK : TOPK + 1], names[:, TOPK + 1 : TOPK + 2]
    home = [lax.shift_right_logical(x, jnp.full_like(x, shift)) for x in picks]
    place = [x & (own - 1) for x in picks]
    lane = lax.broadcasted_iota(jnp.int32, (rows, META), 1)
    member = jnp.where((lane == home[0]) | (lane == home[1]), 1.0, 0.0).astype(BF16)
    ti = lax.broadcasted_iota(jnp.int32, (rows, rows), 0)
    tj = lax.broadcasted_iota(jnp.int32, (rows, rows), 1)
    before = jnp.where(ti > tj, 1.0, 0.0).astype(BF16)
    count = jnp.dot(before, member, preferred_element_type=F32)
    rank = [jnp.sum(jnp.where(lane == x, count, 0.0), axis=1, keepdims=True) for x in home]
    lead = jax.nn.sigmoid(logit)
    mixing = [gain * lead, gain * (1.0 - lead)]
    high = [x.astype(BF16).astype(F32) for x in mixing]
    low = [x - y for x, y in zip(mixing, high)]
    columns = [x.astype(F32) for x in home] + rank + [x.astype(F32) for x in place] + high + low
    meta = jnp.zeros((rows, META), F32)
    for number, column in enumerate(columns):
        meta = jnp.where(lane == number, column, meta)
    block_ref[:, width:] = meta.astype(BF16)
    dispatch_kernel(peers, slots, me_ref, block_ref, *out_refs)


def prepare(own, peers, slots, me, tokens, scale, index, weight, logit):
    rows, width = tokens.shape
    gains = jnp.stack([weight, logit] + [jnp.zeros_like(weight)] * 4)
    inputs = (tokens, scale.reshape(1, -1), index.T, gains)
    full = lambda *shape: pl.BlockSpec(shape, lambda x: (0,) * len(shape))
    block = jax.ShapeDtypeStruct((rows, width + META), BF16)
    return pl.pallas_call(
        functools.partial(prepare_kernel, own, peers, slots),
        grid=(1,),
        in_specs=[SMEM] + [full(*x.shape) for x in inputs],
        out_specs=[full(rows, width + META)] + [full(slots, width + META)] * peers,
        out_shape=[block] + [jax.ShapeDtypeStruct((slots, width + META), BF16)] * peers,
        cost_estimate=cost(2 * peers * slots * rows * width, rows * width * 8),
        name="prepare",
    )(me, *inputs)


def placement(me, meta, total, slots):
    rows = meta.shape[0]
    lane = lax.broadcasted_iota(jnp.int32, (rows, total), 1)
    home = [meta[:, x : x + 1].astype(jnp.int32) for x in (0, 1)]
    rank = [meta[:, x : x + 1].astype(jnp.int32) for x in (2, 3)]
    spot = [(x ^ me) * slots + y for x, y in zip(home, rank)]
    return jnp.where((lane == spot[0]) | (lane == spot[1]), 1.0, 0.0)


def dispatch_kernel(peers, slots, me_ref, block_ref, *out_refs):
    width = block_ref.shape[1] - META
    meta = block_ref[:, width:].astype(F32)
    pick = jnp.transpose(placement(me_ref[0], meta, peers * slots, slots)).astype(BF16)
    for number, out_ref in enumerate(out_refs):
        part = pick[number * slots : (number + 1) * slots, :]
        out_ref[...] = jnp.dot(part, block_ref[...], preferred_element_type=F32).astype(BF16)


def dispatch(peers, slots, me, block):
    rows, width = block.shape
    return pl.pallas_call(
        functools.partial(dispatch_kernel, peers, slots),
        in_specs=[SMEM, VMEM],
        out_specs=[VMEM] * peers,
        out_shape=[jax.ShapeDtypeStruct((slots, width), BF16)] * peers,
        compiler_params=room(8),
        cost_estimate=cost(2 * peers * slots * rows * width, (rows + peers * slots) * width * 2),
        name="dispatch",
    )(me, block)


def expert_kernel(peers, slots, me_ref, *refs):
    x_refs, sources, refs = refs[:peers], refs[peers : peers + 6], refs[peers + 6 :]
    out_refs, (x_all, hidden, *kept, ready) = refs[:peers], refs[peers:]
    gate_a, gate_b, up_a, up_b, down_a, down_b = kept
    own, half, width = gate_a.shape
    units = 2 * half
    rows = peers * slots
    tile = 256

    def fetch(which, expert):
        return pltpu.make_async_copy(
            sources[which].at[expert], kept[which].at[expert], ready.at[which, expert]
        )

    for expert in range(own):
        for which in range(4):
            fetch(which, expert).start()
    for expert in range(own):
        for which in (4, 5):
            fetch(which, expert).start()
    for number, x_ref in enumerate(x_refs):
        x_all[number * slots : (number + 1) * slots, :] = x_ref[...]
    meta = x_all[:, width:].astype(F32)
    me = me_ref[0].astype(F32)

    def inward(expert, carry):
        for which in range(4):
            fetch(which, expert).wait()
        here = expert.astype(F32)
        weight = jnp.zeros((rows, 1), F32)
        for choice in range(TOPK):
            fits = (meta[:, choice : choice + 1] == me) & (meta[:, 4 + choice : 5 + choice] == here)
            value = meta[:, 6 + choice : 7 + choice] + meta[:, 8 + choice : 9 + choice]
            weight = weight + jnp.where(fits, value, 0.0)
        inner = jnp.concatenate([gate_a[expert], gate_b[expert], up_a[expert], up_b[expert]], axis=0)
        both = lax.dot_general(
            x_all[:, :width], inner, (((1,), (1,)), ((), ())), preferred_element_type=F32
        )
        gating, upward = both[:, :units], both[:, units:]
        hidden[expert] = (gating / (1.0 + jnp.exp(-gating)) * upward * weight).astype(BF16)
        return carry

    lax.fori_loop(0, own, inward, 0)
    for expert in range(own):
        for which in (4, 5):
            fetch(which, expert).wait()

    def outward(step, carry):
        span = pl.ds(pl.multiple_of(step * tile, tile), tile)
        left = jnp.concatenate([hidden[x] for x in range(own)], axis=1)
        right = jnp.concatenate(
            [y for x in range(own) for y in (down_a[x, :, span], down_b[x, :, span])], axis=0
        )
        part = jnp.dot(left, right, preferred_element_type=F32).astype(BF16)
        for number, out_ref in enumerate(out_refs):
            out_ref[:, span] = part[number * slots : (number + 1) * slots, :]
        return carry

    lax.fori_loop(0, width // tile, outward, 0)


def expert_part(peers, slots, me, arrived, weights):
    own, units, width = weights[0].shape
    rows = peers * slots
    return pl.pallas_call(
        functools.partial(expert_kernel, peers, slots),
        in_specs=[SMEM] + [VMEM] * peers + [HBM] * 6,
        out_specs=[VMEM] * peers,
        out_shape=[jax.ShapeDtypeStruct((slots, width), BF16)] * peers,
        scratch_shapes=[pltpu.VMEM((rows, width + META), BF16), pltpu.VMEM((own, rows, 2 * units), BF16)]
        + [pltpu.VMEM((own, units, width), BF16)] * 6
        + [pltpu.SemaphoreType.DMA((6, own))],
        compiler_params=room(28),
        cost_estimate=cost(12 * own * units * rows * width, 12 * own * units * width + 4 * rows * width),
        name="expert_part",
    )(me, *arrived, *weights)


def collect_kernel(peers, slots, me_ref, meta_ref, *refs):
    pick = placement(me_ref[0], meta_ref[...].astype(F32), peers * slots, slots).astype(BF16)
    back = jnp.concatenate([x[...] for x in refs[:peers]], axis=0)
    found = jnp.dot(pick, back, preferred_element_type=F32)
    for extra in refs[peers:-1]:
        found = found + extra[...].astype(F32)
    refs[-1][...] = found.astype(BF16)


def collect(peers, slots, me, block, returned, extra):
    rows = block.shape[0]
    width = block.shape[1] - META
    full = lambda *shape: pl.BlockSpec(shape, lambda x: (0,) * len(shape))
    return pl.pallas_call(
        functools.partial(collect_kernel, peers, slots),
        grid=(1,),
        in_specs=[SMEM, pl.BlockSpec((rows, META), lambda x: (0, width // META))]
        + [full(slots, width)] * peers
        + [full(rows, width)] * len(extra),
        out_specs=full(rows, width),
        out_shape=jax.ShapeDtypeStruct((rows, width), BF16),
        compiler_params=room(8),
        cost_estimate=cost(2 * rows * peers * slots * width, (2 * rows + peers * slots) * width * 2),
        name="collect",
    )(me, block, *returned, *extra)


def shards(
    query_heads_rows,
    key_heads_rows,
    value_heads_rows,
    write_strength_logit,
    decay_preactivation,
    head_decay_logarithm,
    extra_log_decay,
    output_weight,
    second_batch_tokens,
    expert_norm_scale,
    expert_choice_index,
    group_router_weight,
    expert_logit_difference,
    expert_gate_weight,
    expert_up_weight,
    expert_down_weight,
):
    ep, tp = lax.axis_size("ep"), lax.axis_size("tp")
    depth = tp // CORES
    me = lax.axis_index("ep")
    rank = lax.axis_index("tp")
    level, core = rank // CORES, rank % CORES
    pair = [(x, x ^ 1) for x in range(tp)]

    def swap(x):
        return lax.ppermute(x, "tp", pair)

    def send(x, chips):
        return lax.ppermute(x, "tp", [(y, (y + chips * CORES) % tp) for y in range(tp)])

    def trade(x, distance):
        return lax.ppermute(x, "ep", [(y, y ^ distance) for y in range(ep)])

    def scalar(x):
        return x.astype(jnp.int32).reshape(1)

    me1 = scalar(me)
    own = EXPERTS // ep
    tokens = second_batch_tokens.shape[0]
    slots = own * CAP // TOPK if own % EPG == 0 else min(own * CAP, tokens)

    block, *sent = prepare(
        own,
        ep,
        slots,
        me1,
        second_batch_tokens,
        expert_norm_scale,
        expert_choice_index,
        group_router_weight,
        expert_logit_difference,
    )
    blocks, arrived = [block], []

    def move(hop):
        return send(blocks[hop - 1], 1)

    def exchange(sent):
        return [sent[0]] + [trade(sent[x], x) for x in range(1, ep)]

    def give_back(produced):
        return [produced[0]] + [trade(produced[x], x) for x in range(1, ep)]

    weights = []
    for shard in (expert_gate_weight, expert_up_weight, expert_down_weight):
        weights += [shard, swap(shard)]
    out_pair = swap(output_weight)

    for hop in range(depth):
        if hop > 0:
            blocks.append(move(hop))
            sent = dispatch(ep, slots, me1, blocks[hop])
        arrived.append(exchange(sent))

    heads = head_decay_logarithm.shape[0]
    local, proj, ends = [], [], []
    for head in range(heads):
        x, y, end = mixer_local(
            head,
            head_decay_logarithm,
            query_heads_rows,
            key_heads_rows,
            value_heads_rows,
            write_strength_logit,
            decay_preactivation,
            extra_log_decay,
        )
        local.append(x)
        proj.append(y)
        ends.append(end)
    joint = jnp.stack(ends)
    joint, weights = lax.optimization_barrier((joint, weights))
    eye = jnp.concatenate([jnp.zeros((DK, DV), F32), jnp.eye(DK, dtype=F32)], axis=1)
    inner = jnp.broadcast_to(eye, joint.shape)
    span = 1
    while True:
        late = scalar((me // span) % 2)
        final = 2 * span >= ep
        got = trade(joint[..., :DV] if final else joint, span)
        if final:
            break
        joint, inner = join(late, joint, got, inner)
        span *= 2
    mine, other = attend(depth, late, scalar(core), local, proj, got, inner)
    theirs = swap(other)
    partial = project(mine, theirs, output_weight, out_pair)

    def piece(hop):
        at = (level + depth - hop) % depth
        return lax.dynamic_index_in_dim(partial, at, 0, keepdims=False)

    mixed = piece(0).astype(F32)
    for hop in range(1, depth):
        mixed = mixed + send(piece(hop), -hop).astype(F32)

    found = []
    for hop in range(depth):
        produced = expert_part(ep, slots, me1, arrived[hop], weights)
        found.append(give_back(produced))
    running, near = [], []
    for hop in range(1, depth):
        total = collect(ep, slots, me1, blocks[hop], found[hop], running)
        if hop == 1:
            near = [send(total, -1)]
        else:
            running = [send(total, 1)]
    expert_out = collect(ep, slots, me1, blocks[0], found[0], near + running)
    return (mixed.astype(BF16), expert_out)


def solution(mesh):
    in_specs = (
        P("ep", "tp"),
        P("ep", "tp"),
        P("ep", "tp"),
        P("tp", "ep"),
        P("tp", "ep"),
        P("tp"),
        P("tp", "ep"),
        P("tp", None),
        P(("ep", "tp"), None),
        P(),
        P(("ep", "tp"), None),
        P(("ep", "tp")),
        P(("ep", "tp")),
        P("ep", "tp", None),
        P("ep", "tp", None),
        P("ep", "tp", None),
    )
    out_specs = (P(("ep", "tp"), None), P(("ep", "tp"), None))

    return jax.shard_map(shards, mesh=mesh, in_specs=in_specs, out_specs=out_specs, check_vma=False)
```

```python
import functools

import jax
import jax.numpy as jnp
from jax import lax
from jax.experimental import pallas as pl
from jax.experimental.pallas import tpu as pltpu
from jax.sharding import PartitionSpec as P


DK = 128
DV = 128
CAP = 32
EXPERTS = 16
EPG = 4
TOPK = 2
CORES = 2
META = 128
CHUNK = 128
FIRST_ROOM, EXPERT_ROOM = 64000 * 1024, 24 * 2**20
FETCH = (1,)
NORM_EPS = 1e-06


F32 = jnp.float32
BF16 = jnp.bfloat16
EXACT = lax.Precision.HIGHEST
VMEM = pl.BlockSpec(memory_space=pltpu.VMEM)
HBM = pl.BlockSpec(memory_space=pltpu.HBM)
SMEM = pl.BlockSpec(memory_space=pltpu.SMEM)


def room(mib):
    return pltpu.CompilerParams(vmem_limit_bytes=mib * 2**20)


def cost(flops, moved):
    return pl.CostEstimate(flops=int(flops), bytes_accessed=int(moved), transcendentals=0)


def mm(a, b):
    return jnp.dot(a, b, precision=EXACT, preferred_element_type=F32)


def halves(x):
    high = x.astype(BF16)
    return high, (x - high.astype(F32)).astype(BF16)


def mm3(a, b):
    (ah, al), (bh, bl) = halves(a), halves(b)
    dot = lambda x, y: jnp.dot(x, y, preferred_element_type=F32)
    return dot(ah, bh) + (dot(ah, bl) + dot(al, bh))


def mixer_kernel(head, rate_ref, q_ref, k_ref, v_ref, write_ref, decay_ref, extra_ref, *refs):
    early_refs, (local_ref, proj_ref, joint_ref) = refs[:-3], refs[-3:]
    length = q_ref.shape[0]
    chunks = length // CHUNK
    i = lax.broadcasted_iota(jnp.int32, (CHUNK, CHUNK), 0)
    j = lax.broadcasted_iota(jnp.int32, (CHUNK, CHUNK), 1)
    every = range(chunks)
    spans = [slice(c * CHUNK, (c + 1) * CHUNK) for c in every]

    def unit(ref, n):
        x = ref[spans[n], :].astype(F32)
        return x * lax.rsqrt(jnp.sum(x * x, axis=-1, keepdims=True) + NORM_EPS)

    q = [unit(q_ref, n) * DK**-0.5 for n in every]
    k = [unit(k_ref, n) for n in every]
    kt = [jnp.transpose(x) for x in k]
    v = [v_ref[spans[n], :].astype(F32) for n in every]
    raised = decay_ref[head : head + 1, :].astype(F32)
    soft = jnp.maximum(raised, 0.0) + jnp.log(1.0 + jnp.exp(-jnp.abs(raised)))
    rate = jnp.exp(jnp.full((1, length), rate_ref[head], F32))
    drops = extra_ref[head : head + 1, :] - rate * soft
    writes = jax.nn.sigmoid(write_ref[head : head + 1, :].astype(F32))
    drops = jnp.concatenate([drops[:, x] for x in spans], axis=0)
    writes = jnp.concatenate([writes[:, x] for x in spans], axis=0)
    summed = mm(drops, jnp.where(i <= j, 1.0, 0.0))
    columns = jnp.transpose(jnp.concatenate([summed, writes], axis=0))
    row = [summed[n : n + 1, :] for n in every]
    col = [columns[:, n : n + 1] for n in every]
    beta = [columns[:, len(every) + n : len(every) + n + 1] for n in every]
    last = [r[:, CHUNK - 1 :] for r in row]
    decay = [jnp.where(i >= j, jnp.exp(jnp.where(i >= j, col[n] - row[n], 0.0)), 0.0) for n in every]
    gram = [mm3(k[n], kt[n]) for n in every]
    lower = [jnp.where(i > j, gram[n] * decay[n] * beta[n], 0.0) for n in every]
    scores = [mm3(q[n], kt[n]) * decay[n] for n in every]
    eye = jnp.where(i == j, 1.0, 0.0)
    small = 16
    near = (i // small) == (j // small)
    power = [jnp.where(near, x, 0.0) for x in lower]
    inverse = [eye - x for x in power]
    reach = 2
    while reach < small:
        power = [mm3(x, x) for x in power]
        inverse = [x + mm3(x, y) for x, y in zip(inverse, power)]
        reach *= 2
    while small < CHUNK:
        band = ((i // (2 * small)) == (j // (2 * small))) & ((i // small) != (j // small))
        half = [mm3(jnp.where(band, x, 0.0), y) for x, y in zip(lower, inverse)]
        inverse = [y - mm3(y, x) for x, y in zip(half, inverse)]
        small *= 2
    grown = [jnp.exp(x) for x in col]
    rhs = [jnp.concatenate([v[n] * beta[n], k[n] * (beta[n] * grown[n])], axis=1) for n in every]
    solved = [mm3(inverse[n], rhs[n]) for n in every]
    blank = jnp.zeros((CHUNK, DK), F32)
    start = jnp.concatenate([jnp.zeros((DK, DV), F32), eye], axis=1)
    joint = start
    for n in every:
        update = jnp.concatenate([solved[n][:, :DV], blank], axis=1) - mm3(solved[n][:, DV:], joint)
        out = mm3(q[n] * grown[n], joint) + mm3(scores[n], update)
        joint = joint * jnp.exp(last[n]) + mm3(kt[n] * jnp.exp(last[n] - row[n]), update)
        local_ref[spans[n], :] = out[:, :DV]
        proj_ref[spans[n], :] = out[:, DV:]
    for number, early_ref in enumerate(early_refs):
        joint_ref[number] = early_ref[0]
    joint_ref[len(early_refs)] = joint


def mixer_local(head, rates, queries, keys, values, write, decay, extra, early):
    length = queries.shape[0]
    tall = pl.BlockSpec((length, DK), lambda x: (0, head))
    gate = pl.BlockSpec(write.shape, lambda x: (0, 0))
    flat = pl.BlockSpec((length, DK), lambda x: (0, 0))
    ends = lambda n: pl.BlockSpec((n, DK, DV + DK), lambda x: (0, 0, 0))
    return pl.pallas_call(
        functools.partial(mixer_kernel, head),
        grid=(1,),
        in_specs=[SMEM] + [tall] * 3 + [gate] * 3 + [ends(1)] * len(early),
        out_specs=[flat, flat, ends(1 + len(early))],
        out_shape=[
            jax.ShapeDtypeStruct((length, DV), F32),
            jax.ShapeDtypeStruct((length, DK), F32),
            jax.ShapeDtypeStruct((1 + len(early), DK, DV + DK), F32),
        ],
        cost_estimate=cost(length // CHUNK * 26 * 6 * 2 * 128**3, length * DK * 14),
        name="mixer_local",
    )(rates, queries, keys, values, write, decay, extra, *early)


def join_kernel(late_ref, own_ref, got_ref, inner_ref, own_out, inner_out):
    late = late_ref[0] > 0
    for h in range(own_ref.shape[0]):
        own, got, inner = own_ref[h], got_ref[h], inner_ref[h]
        first, second = jnp.where(late, got, own), jnp.where(late, own, got)
        blank = jnp.zeros_like(own[:, DV:])
        keep = lambda x: jnp.concatenate([x[:, :DV], blank], axis=1)
        own_out[h] = mm(second[:, DV:], first) + keep(second)
        inner_out[h] = jnp.where(late, mm(inner[:, DV:], got) + keep(inner), inner)


def join(late, own, got, inner):
    shape = jax.ShapeDtypeStruct(own.shape, F32)
    return pl.pallas_call(
        join_kernel,
        in_specs=[SMEM] + [VMEM] * 3,
        out_specs=[VMEM] * 2,
        out_shape=[shape, shape],
        compiler_params=room(8),
        cost_estimate=cost(own.size * 24 * DK, own.size * 20),
        name="join",
    )(late, own, got, inner)


def attend_kernel(heads, late_ref, core_ref, *refs):
    local_refs, proj_refs = refs[:heads], refs[heads : 2 * heads]
    got_ref, inner_ref, mine_ref, other_ref = refs[2 * heads :]
    late = late_ref[0] > 0
    states = []
    for h in range(heads):
        inner = inner_ref[h]
        state = mm3(inner[:, DV:], got_ref[h]) + inner[:, :DV]
        states.append(jnp.where(late, state, inner[:, :DV]))
    depth, rows = mine_ref.shape[0], mine_ref.shape[1]
    for out_ref, shift in ((mine_ref, core_ref[0]), (other_ref, 1 - core_ref[0])):
        for z in range(depth):
            span = pl.ds(pl.multiple_of((z * CORES + shift) * rows, rows), rows)
            for h in range(heads):
                out = local_refs[h][span, :] + mm3(proj_refs[h][span, :], states[h])
                out_ref[z, :, h * DV : (h + 1) * DV] = out.astype(BF16)


def attend(depth, late, core, local, proj, got, inner):
    heads = len(local)
    length, width = local[0].shape
    half = jax.ShapeDtypeStruct((depth, length // depth // CORES, heads * width), BF16)
    full = lambda *shape: pl.BlockSpec(shape, lambda x: (0,) * len(shape))
    return pl.pallas_call(
        functools.partial(attend_kernel, heads),
        grid=(1,),
        in_specs=[SMEM] * 2 + [full(length, width)] * (2 * heads) + [full(*got.shape), full(*inner.shape)],
        out_specs=[full(*half.shape)] * 2,
        out_shape=[half, half],
        cost_estimate=cost(6 * 2 * length * width * DK * heads, length * width * 10 * heads),
        name="attend",
    )(late, core, *local, *proj, got, inner)


def project_kernel(level_ref, mine_ref, theirs_ref, own_ref, pair_ref, *refs):
    depth, rows, width = mine_ref.shape
    out_refs, (weight, ready) = refs[:depth], refs[depth:]
    tile = weight.shape[2]
    steps = weight.shape[0]

    def fetch(step, half):
        source = (own_ref, pair_ref)[half]
        return pltpu.make_async_copy(
            source.at[:, pl.ds(step * tile, tile)],
            weight.at[step, pl.ds(half * width, width)],
            ready.at[step, half],
        )

    for step in range(steps):
        for half in range(CORES):
            fetch(step, half).start()
    order = [lax.rem(level_ref[0] + depth - hop, depth) for hop in range(depth)]
    left = jnp.concatenate(
        [jnp.concatenate([mine_ref[at], theirs_ref[at]], axis=1) for at in order], axis=0
    )
    for step in range(steps):
        for half in range(CORES):
            fetch(step, half).wait()
        part = jnp.dot(left, weight[step], preferred_element_type=F32).astype(BF16)
        for hop, out_ref in enumerate(out_refs):
            out_ref[:, step * tile : (step + 1) * tile] = part[hop * rows : (hop + 1) * rows, :]


def project(level, mine, theirs, own, pair):
    depth, rows, width = mine.shape
    wide = own.shape[1]
    tile = 512
    return pl.pallas_call(
        project_kernel,
        in_specs=[SMEM, VMEM, VMEM, HBM, HBM],
        out_specs=[VMEM] * depth,
        out_shape=[jax.ShapeDtypeStruct((rows, wide), BF16)] * depth,
        scratch_shapes=[
            pltpu.VMEM((wide // tile, CORES * width, tile), BF16),
            pltpu.SemaphoreType.DMA((wide // tile, CORES)),
        ],
        compiler_params=room(8),
        cost_estimate=cost(4 * depth * rows * width * wide, 4 * width * wide + 2 * depth * rows * wide),
        name="project",
    )(level, mine, theirs, own, pair)


def prepare_kernel(own, peers, slots, me_ref, x_ref, scale_ref, index_ref, gain_ref, logit_ref, block_ref, *out_refs):
    rows, width = x_ref.shape
    x = x_ref[...].astype(F32)
    inv = lax.rsqrt(jnp.mean(x * x, axis=-1, keepdims=True) + NORM_EPS)
    block_ref[:, :width] = (x * inv * scale_ref[...]).astype(BF16)
    shift = own.bit_length() - 1
    given = [index_ref[...].astype(F32), gain_ref[...], logit_ref[...], jnp.zeros((8 - TOPK - 2, rows), F32)]
    names = jnp.transpose(jnp.concatenate(given, axis=0))
    picks = [names[:, n : n + 1].astype(jnp.int32) for n in range(TOPK)]
    gain, logit = names[:, TOPK : TOPK + 1], names[:, TOPK + 1 : TOPK + 2]
    home = [lax.shift_right_logical(x, jnp.full_like(x, shift)) for x in picks]
    place = [x & (own - 1) for x in picks]
    lane = lax.broadcasted_iota(jnp.int32, (rows, META), 1)
    member = jnp.where((lane == home[0]) | (lane == home[1]), 1.0, 0.0).astype(BF16)
    ti = lax.broadcasted_iota(jnp.int32, (rows, rows), 0)
    tj = lax.broadcasted_iota(jnp.int32, (rows, rows), 1)
    before = jnp.where(ti > tj, 1.0, 0.0).astype(BF16)
    count = jnp.dot(before, member, preferred_element_type=F32)
    rank = [jnp.sum(jnp.where(lane == x, count, 0.0), axis=1, keepdims=True) for x in home]
    lead = jax.nn.sigmoid(logit)
    mixing = [gain * lead, gain * (1.0 - lead)]
    high = [x.astype(BF16).astype(F32) for x in mixing]
    low = [x - y for x, y in zip(mixing, high)]
    columns = [x.astype(F32) for x in home] + rank + [x.astype(F32) for x in place] + high + low
    meta = jnp.zeros((rows, META), F32)
    for number, column in enumerate(columns):
        meta = jnp.where(lane == number, column, meta)
    block_ref[:, width:] = meta.astype(BF16)
    dispatch_kernel(peers, slots, me_ref, block_ref, *out_refs)


def prepare(own, peers, slots, me, tokens, scale, index, weight, logit):
    rows, width = tokens.shape
    inputs = (tokens, scale.reshape(1, -1), index.T, weight.reshape(1, -1), logit.reshape(1, -1))
    full = lambda *shape: pl.BlockSpec(shape, lambda x: (0,) * len(shape))
    block = jax.ShapeDtypeStruct((rows, width + META), BF16)
    return pl.pallas_call(
        functools.partial(prepare_kernel, own, peers, slots),
        grid=(1,),
        in_specs=[SMEM] + [full(*x.shape) for x in inputs],
        out_specs=[full(rows, width + META)] + [full(slots, width + META)] * peers,
        out_shape=[block] + [jax.ShapeDtypeStruct((slots, width + META), BF16)] * peers,
        cost_estimate=cost(2 * peers * slots * rows * width, rows * width * 8),
        name="prepare",
    )(me, *inputs)


def placement(me, meta, total, slots):
    rows = meta.shape[0]
    lane = lax.broadcasted_iota(jnp.int32, (rows, total), 1)
    home = [meta[:, x : x + 1].astype(jnp.int32) for x in (0, 1)]
    rank = [meta[:, x : x + 1].astype(jnp.int32) for x in (2, 3)]
    spot = [(x ^ me) * slots + y for x, y in zip(home, rank)]
    return jnp.where((lane == spot[0]) | (lane == spot[1]), 1.0, 0.0)


def dispatch_kernel(peers, slots, me_ref, block_ref, *out_refs):
    width = block_ref.shape[1] - META
    meta = block_ref[:, width:].astype(F32)
    pick = jnp.transpose(placement(me_ref[0], meta, peers * slots, slots)).astype(BF16)
    for number, out_ref in enumerate(out_refs):
        part = pick[number * slots : (number + 1) * slots, :]
        out_ref[...] = jnp.dot(part, block_ref[...], preferred_element_type=F32).astype(BF16)


def dispatch(peers, slots, me, block):
    rows, width = block.shape
    return pl.pallas_call(
        functools.partial(dispatch_kernel, peers, slots),
        in_specs=[SMEM, VMEM],
        out_specs=[VMEM] * peers,
        out_shape=[jax.ShapeDtypeStruct((slots, width), BF16)] * peers,
        compiler_params=room(8),
        cost_estimate=cost(2 * peers * slots * rows * width, (rows + peers * slots) * width * 2),
        name="dispatch",
    )(me, block)


def expert_kernel(moved, peers, slots, me_ref, *refs):
    x_refs, refs = refs[:peers], refs[peers:]
    sources, out_refs = refs[:6], refs[6 : 6 + peers]
    x_all, hidden, held, ready = refs[6 + peers :]
    kept = [held.at[moved.index(x)] if x in moved else sources[x] for x in range(6)]
    own, half, width = sources[0].shape
    units = 2 * half
    rows = peers * slots
    tile = 512

    def fetch(which, expert):
        return pltpu.make_async_copy(
            sources[which].at[expert], kept[which].at[expert], ready.at[which, expert]
        )

    inner_moved = [x for x in moved if x < 4]
    outer_moved = [x for x in moved if x >= 4]
    for whiches in (inner_moved, outer_moved):
        for expert in range(own):
            for which in whiches:
                fetch(which, expert).start()
    for number, x_ref in enumerate(x_refs):
        x_all[number * slots : (number + 1) * slots, :] = x_ref[...]
    meta = x_all[:, width:].astype(F32)
    me = me_ref[0].astype(F32)

    def inward(expert, carry):
        for which in inner_moved:
            fetch(which, expert).wait()
        here = expert.astype(F32)
        weight = jnp.zeros((rows, 1), F32)
        for choice in range(TOPK):
            fits = (meta[:, choice : choice + 1] == me) & (meta[:, 4 + choice : 5 + choice] == here)
            value = meta[:, 6 + choice : 7 + choice] + meta[:, 8 + choice : 9 + choice]
            weight = weight + jnp.where(fits, value, 0.0)
        inner = jnp.concatenate([kept[x][expert] for x in range(4)], axis=0)
        both = lax.dot_general(
            x_all[:, :width], inner, (((1,), (1,)), ((), ())), preferred_element_type=F32
        )
        gating, upward = both[:, :units], both[:, units:]
        hidden[expert] = (gating / (1.0 + jnp.exp(-gating)) * upward * weight).astype(BF16)
        return carry

    lax.fori_loop(0, own, inward, 0)
    for expert in range(own):
        for which in outer_moved:
            fetch(which, expert).wait()

    def outward(step, carry):
        span = pl.ds(pl.multiple_of(step * tile, tile), tile)
        left = jnp.concatenate([hidden[x] for x in range(own)], axis=1)
        right = jnp.concatenate([kept[y][x, :, span] for x in range(own) for y in (4, 5)], axis=0)
        part = jnp.dot(left, right, preferred_element_type=F32).astype(BF16)
        for number, out_ref in enumerate(out_refs):
            out_ref[:, span] = part[number * slots : (number + 1) * slots, :]
        return carry

    lax.fori_loop(0, width // tile, outward, 0)


def expert_part(first, peers, slots, me, arrived, weights):
    own, units, width = weights[0].shape[-3:]
    rows = peers * slots
    moved = tuple(range(6)) if first else (1, 3, 5)
    return pl.pallas_call(
        functools.partial(expert_kernel, moved, peers, slots),
        in_specs=[SMEM] + [VMEM] * peers + [HBM if x in moved else VMEM for x in range(6)],
        out_specs=[VMEM] * peers,
        out_shape=[jax.ShapeDtypeStruct((slots, width), BF16)] * peers,
        scratch_shapes=[
            pltpu.VMEM((rows, width + META), BF16),
            pltpu.VMEM((own, rows, 2 * units), BF16),
            pltpu.VMEM((len(moved), own, units, width), BF16),
            pltpu.SemaphoreType.DMA((6, own)),
        ],
        compiler_params=pltpu.CompilerParams(vmem_limit_bytes=FIRST_ROOM if first else EXPERT_ROOM),
        cost_estimate=cost(12 * own * units * rows * width, 12 * own * units * width + 4 * rows * width),
        name="expert_part",
    )(me, *arrived, *weights)


def collect_kernel(peers, slots, me_ref, meta_ref, *refs):
    pick = placement(me_ref[0], meta_ref[...].astype(F32), peers * slots, slots).astype(BF16)
    back = jnp.concatenate([x[...] for x in refs[:peers]], axis=0)
    found = jnp.dot(pick, back, preferred_element_type=F32)
    for extra in refs[peers:-1]:
        found = found + extra[...].astype(F32)
    refs[-1][...] = found.astype(BF16)


def collect(peers, slots, me, block, returned, extra):
    rows = block.shape[0]
    width = block.shape[1] - META
    full = lambda *shape: pl.BlockSpec(shape, lambda x: (0,) * len(shape))
    return pl.pallas_call(
        functools.partial(collect_kernel, peers, slots),
        grid=(1,),
        in_specs=[SMEM, pl.BlockSpec((rows, META), lambda x: (0, width // META))]
        + [full(slots, width)] * peers
        + [full(rows, width)] * len(extra),
        out_specs=full(rows, width),
        out_shape=jax.ShapeDtypeStruct((rows, width), BF16),
        compiler_params=room(8),
        cost_estimate=cost(2 * rows * peers * slots * width, (2 * rows + peers * slots) * width * 2),
        name="collect",
    )(me, block, *returned, *extra)


def shards(
    query_heads_rows,
    key_heads_rows,
    value_heads_rows,
    write_strength_logit,
    decay_preactivation,
    head_decay_logarithm,
    extra_log_decay,
    output_weight,
    second_batch_tokens,
    expert_norm_scale,
    expert_choice_index,
    group_router_weight,
    expert_logit_difference,
    expert_gate_weight,
    expert_up_weight,
    expert_down_weight,
):
    ep, tp = lax.axis_size("ep"), lax.axis_size("tp")
    depth = tp // CORES
    me = lax.axis_index("ep")
    rank = lax.axis_index("tp")
    level, core = rank // CORES, rank % CORES
    pair = [(x, x ^ 1) for x in range(tp)]

    def swap(x):
        return lax.ppermute(x, "tp", pair)

    def send(x, chips):
        return lax.ppermute(x, "tp", [(y, (y + chips * CORES) % tp) for y in range(tp)])

    def trade(x, distance):
        return lax.ppermute(x, "ep", [(y, y ^ distance) for y in range(ep)])

    def scalar(x):
        return x.astype(jnp.int32).reshape(1)

    me1 = scalar(me)
    own = EXPERTS // ep
    tokens = second_batch_tokens.shape[0]
    slots = own * CAP // TOPK if own % EPG == 0 else min(own * CAP, tokens)

    block, *sent = prepare(
        own,
        ep,
        slots,
        me1,
        second_batch_tokens,
        expert_norm_scale,
        expert_choice_index,
        group_router_weight,
        expert_logit_difference,
    )
    blocks, arrived = [block], []

    def move(hop):
        return send(blocks[hop - 1], 1)

    def exchange(sent):
        return [sent[0]] + [trade(sent[x], x) for x in range(1, ep)]

    def give_back(produced):
        return [produced[0]] + [trade(produced[x], x) for x in range(1, ep)]

    weights = []
    for shard in (expert_gate_weight, expert_up_weight, expert_down_weight):
        weights += [shard, swap(shard)]
    out_pair = swap(output_weight)

    for hop in range(depth):
        if hop > 0:
            blocks.append(move(hop))
            sent = dispatch(ep, slots, me1, blocks[hop])
        arrived.append(exchange(sent))

    heads = head_decay_logarithm.shape[0]
    local, proj, ends = [], [], []
    for head in range(heads):
        x, y, end = mixer_local(
            head,
            head_decay_logarithm,
            query_heads_rows,
            key_heads_rows,
            value_heads_rows,
            write_strength_logit,
            decay_preactivation,
            extra_log_decay,
            ends if head == heads - 1 else [],
        )
        local.append(x)
        proj.append(y)
        ends.append(end)
    joint = ends[-1]
    joint, weights = lax.optimization_barrier((joint, weights))
    eye = jnp.concatenate([jnp.zeros((DK, DV), F32), jnp.eye(DK, dtype=F32)], axis=1)
    inner = jnp.broadcast_to(eye, joint.shape)
    span = 1
    while True:
        late = scalar((me // span) % 2)
        final = 2 * span >= ep
        got = trade(joint[..., :DV] if final else joint, span)
        if final:
            break
        joint, inner = join(late, joint, got, inner)
        span *= 2
    mine, other = attend(depth, late, scalar(core), local, proj, got, inner)
    theirs = swap(other)
    pieces = project(scalar(level), mine, theirs, output_weight, out_pair)

    mixed = pieces[0].astype(F32)
    for hop in range(1, depth):
        mixed = mixed + send(pieces[hop], -hop).astype(F32)

    found = {}
    for hop in list(range(1, depth)) + [0]:
        produced = expert_part(hop in FETCH, ep, slots, me1, arrived[hop], weights)
        found[hop] = give_back(produced)
    running, near = [], []
    for hop in range(1, depth):
        total = collect(ep, slots, me1, blocks[hop], found[hop], running)
        if hop == 1:
            near = [send(total, -1)]
        else:
            running = [send(total, 1)]
    expert_out = collect(ep, slots, me1, blocks[0], found[0], near)
    if running:
        expert_out = (expert_out.astype(F32) + running[0].astype(F32)).astype(BF16)
    return (mixed.astype(BF16), expert_out)


def solution(mesh):
    in_specs = (
        P("ep", "tp"),
        P("ep", "tp"),
        P("ep", "tp"),
        P("tp", "ep"),
        P("tp", "ep"),
        P("tp"),
        P("tp", "ep"),
        P("tp", None),
        P(("ep", "tp"), None),
        P(),
        P(("ep", "tp"), None),
        P(("ep", "tp")),
        P(("ep", "tp")),
        P("ep", "tp", None),
        P("ep", "tp", None),
        P("ep", "tp", None),
    )
    out_specs = (P(("ep", "tp"), None), P(("ep", "tp"), None))

    return jax.shard_map(shards, mesh=mesh, in_specs=in_specs, out_specs=out_specs, check_vma=False)
```

```python
import functools

import jax
import jax.numpy as jnp
from jax import lax
from jax.experimental import pallas as pl
from jax.experimental.pallas import tpu as pltpu
from jax.sharding import PartitionSpec as P


DK = 128
DV = 128
CAP = 32
EXPERTS = 16
EPG = 4
TOPK = 2
CORES = 2
META = 128
CHUNK = 128
FIRST_ROOM, EXPERT_ROOM = 64000 * 1024, 24 * 2**20
FETCH = (1,)
NORM_EPS = 1e-06


F32 = jnp.float32
BF16 = jnp.bfloat16
EXACT = lax.Precision.HIGHEST
VMEM = pl.BlockSpec(memory_space=pltpu.VMEM)
HBM = pl.BlockSpec(memory_space=pltpu.HBM)
SMEM = pl.BlockSpec(memory_space=pltpu.SMEM)


def room(mib):
    return pltpu.CompilerParams(vmem_limit_bytes=mib * 2**20)


def cost(flops, moved):
    return pl.CostEstimate(flops=int(flops), bytes_accessed=int(moved), transcendentals=0)


def mm(a, b):
    return jnp.dot(a, b, precision=EXACT, preferred_element_type=F32)


def halves(x):
    high = x.astype(BF16)
    return high, (x - high.astype(F32)).astype(BF16)


def mm3(a, b):
    (ah, al), (bh, bl) = halves(a), halves(b)
    dot = lambda x, y: jnp.dot(x, y, preferred_element_type=F32)
    return dot(ah, bh) + (dot(ah, bl) + dot(al, bh))


def mixer_kernel(head, rate_ref, q_ref, k_ref, v_ref, write_ref, decay_ref, extra_ref, *refs):
    early_refs, (local_ref, proj_ref, joint_ref) = refs[:-3], refs[-3:]
    length = q_ref.shape[0]
    chunks = length // CHUNK
    i = lax.broadcasted_iota(jnp.int32, (CHUNK, CHUNK), 0)
    j = lax.broadcasted_iota(jnp.int32, (CHUNK, CHUNK), 1)
    every = range(chunks)
    spans = [slice(c * CHUNK, (c + 1) * CHUNK) for c in every]

    def unit(ref, n):
        x = ref[spans[n], :].astype(F32)
        return x * lax.rsqrt(jnp.sum(x * x, axis=-1, keepdims=True) + NORM_EPS)

    q = [unit(q_ref, n) * DK**-0.5 for n in every]
    k = [unit(k_ref, n) for n in every]
    kt = [jnp.transpose(x) for x in k]
    v = [v_ref[spans[n], :].astype(F32) for n in every]
    raised = decay_ref[head : head + 1, :].astype(F32)
    soft = jnp.maximum(raised, 0.0) + jnp.log(1.0 + jnp.exp(-jnp.abs(raised)))
    rate = jnp.exp(jnp.full((1, length), rate_ref[head], F32))
    drops = extra_ref[head : head + 1, :] - rate * soft
    writes = jax.nn.sigmoid(write_ref[head : head + 1, :].astype(F32))
    drops = jnp.concatenate([drops[:, x] for x in spans], axis=0)
    writes = jnp.concatenate([writes[:, x] for x in spans], axis=0)
    summed = mm(drops, jnp.where(i <= j, 1.0, 0.0))
    columns = jnp.transpose(jnp.concatenate([summed, writes], axis=0))
    row = [summed[n : n + 1, :] for n in every]
    col = [columns[:, n : n + 1] for n in every]
    beta = [columns[:, len(every) + n : len(every) + n + 1] for n in every]
    last = [r[:, CHUNK - 1 :] for r in row]
    decay = [jnp.where(i >= j, jnp.exp(jnp.where(i >= j, col[n] - row[n], 0.0)), 0.0) for n in every]
    gram = [mm3(k[n], kt[n]) for n in every]
    lower = [jnp.where(i > j, gram[n] * decay[n] * beta[n], 0.0) for n in every]
    scores = [mm3(q[n], kt[n]) * decay[n] for n in every]
    eye = jnp.where(i == j, 1.0, 0.0)
    small = 16
    near = (i // small) == (j // small)
    power = [jnp.where(near, x, 0.0) for x in lower]
    inverse = [eye - x for x in power]
    reach = 2
    while reach < small:
        power = [mm3(x, x) for x in power]
        inverse = [x + mm3(x, y) for x, y in zip(inverse, power)]
        reach *= 2
    while small < CHUNK:
        band = ((i // (2 * small)) == (j // (2 * small))) & ((i // small) != (j // small))
        half = [mm3(jnp.where(band, x, 0.0), y) for x, y in zip(lower, inverse)]
        inverse = [y - mm3(y, x) for x, y in zip(half, inverse)]
        small *= 2
    grown = [jnp.exp(x) for x in col]
    rhs = [jnp.concatenate([v[n] * beta[n], k[n] * (beta[n] * grown[n])], axis=1) for n in every]
    solved = [mm3(inverse[n], rhs[n]) for n in every]
    blank = jnp.zeros((CHUNK, DK), F32)
    start = jnp.concatenate([jnp.zeros((DK, DV), F32), eye], axis=1)
    joint = start
    for n in every:
        update = jnp.concatenate([solved[n][:, :DV], blank], axis=1) - mm3(solved[n][:, DV:], joint)
        out = mm3(q[n] * grown[n], joint) + mm3(scores[n], update)
        joint = joint * jnp.exp(last[n]) + mm3(kt[n] * jnp.exp(last[n] - row[n]), update)
        local_ref[spans[n], :] = out[:, :DV]
        proj_ref[spans[n], :] = out[:, DV:].astype(BF16)
    for number, early_ref in enumerate(early_refs):
        joint_ref[number] = early_ref[0]
    joint_ref[len(early_refs)] = joint


def mixer_local(head, rates, queries, keys, values, write, decay, extra, early):
    length = queries.shape[0]
    tall = pl.BlockSpec((length, DK), lambda x: (0, head))
    gate = pl.BlockSpec(write.shape, lambda x: (0, 0))
    flat = pl.BlockSpec((length, DK), lambda x: (0, 0))
    ends = lambda n: pl.BlockSpec((n, DK, DV + DK), lambda x: (0, 0, 0))
    return pl.pallas_call(
        functools.partial(mixer_kernel, head),
        grid=(1,),
        in_specs=[SMEM] + [tall] * 3 + [gate] * 3 + [ends(1)] * len(early),
        out_specs=[flat, flat, ends(1 + len(early))],
        out_shape=[
            jax.ShapeDtypeStruct((length, DV), F32),
            jax.ShapeDtypeStruct((length, DK), BF16),
            jax.ShapeDtypeStruct((1 + len(early), DK, DV + DK), F32),
        ],
        cost_estimate=cost(length // CHUNK * 26 * 6 * 2 * 128**3, length * DK * 14),
        name="mixer_local",
    )(rates, queries, keys, values, write, decay, extra, *early)


def join_kernel(late_ref, own_ref, got_ref, inner_ref, own_out, inner_out):
    late = late_ref[0] > 0
    for h in range(own_ref.shape[0]):
        own, got, inner = own_ref[h], got_ref[h], inner_ref[h]
        first, second = jnp.where(late, got, own), jnp.where(late, own, got)
        blank = jnp.zeros_like(own[:, DV:])
        keep = lambda x: jnp.concatenate([x[:, :DV], blank], axis=1)
        own_out[h] = mm(second[:, DV:], first) + keep(second)
        inner_out[h] = jnp.where(late, mm(inner[:, DV:], got) + keep(inner), inner)


def join(late, own, got, inner):
    shape = jax.ShapeDtypeStruct(own.shape, F32)
    return pl.pallas_call(
        join_kernel,
        in_specs=[SMEM] + [VMEM] * 3,
        out_specs=[VMEM] * 2,
        out_shape=[shape, shape],
        compiler_params=room(8),
        cost_estimate=cost(own.size * 24 * DK, own.size * 20),
        name="join",
    )(late, own, got, inner)


def attend_kernel(heads, late_ref, core_ref, *refs):
    local_refs, proj_refs = refs[:heads], refs[heads : 2 * heads]
    got_ref, inner_ref, mine_ref, other_ref = refs[2 * heads :]
    late = late_ref[0] > 0
    states = []
    for h in range(heads):
        inner = inner_ref[h]
        state = mm3(inner[:, DV:], got_ref[h]) + inner[:, :DV]
        states.append(jnp.concatenate(halves(jnp.where(late, state, inner[:, :DV])), axis=1))
    depth, rows = mine_ref.shape[0], mine_ref.shape[1]
    for out_ref, shift in ((mine_ref, core_ref[0]), (other_ref, 1 - core_ref[0])):
        for z in range(depth):
            span = pl.ds(pl.multiple_of((z * CORES + shift) * rows, rows), rows)
            for h in range(heads):
                both = jnp.dot(proj_refs[h][span, :], states[h], preferred_element_type=F32)
                out = local_refs[h][span, :] + both[:, :DV] + both[:, DV:]
                out_ref[z, :, h * DV : (h + 1) * DV] = out.astype(BF16)


def attend(depth, late, core, local, proj, got, inner):
    heads = len(local)
    length, width = local[0].shape
    half = jax.ShapeDtypeStruct((depth, length // depth // CORES, heads * width), BF16)
    full = lambda *shape: pl.BlockSpec(shape, lambda x: (0,) * len(shape))
    return pl.pallas_call(
        functools.partial(attend_kernel, heads),
        grid=(1,),
        in_specs=[SMEM] * 2 + [full(length, width)] * (2 * heads) + [full(*got.shape), full(*inner.shape)],
        out_specs=[full(*half.shape)] * 2,
        out_shape=[half, half],
        cost_estimate=cost(6 * 2 * length * width * DK * heads, length * width * 10 * heads),
        name="attend",
    )(late, core, *local, *proj, got, inner)


def project_kernel(level_ref, mine_ref, theirs_ref, own_ref, pair_ref, *refs):
    depth, rows, width = mine_ref.shape
    out_refs, (weight, ready) = refs[:depth], refs[depth:]
    tile = weight.shape[2]
    steps = weight.shape[0]

    def fetch(step, half):
        source = (own_ref, pair_ref)[half]
        return pltpu.make_async_copy(
            source.at[:, pl.ds(step * tile, tile)],
            weight.at[step, pl.ds(half * width, width)],
            ready.at[step, half],
        )

    for step in range(steps):
        for half in range(CORES):
            fetch(step, half).start()
    order = [lax.rem(level_ref[0] + depth - hop, depth) for hop in range(depth)]
    left = jnp.concatenate(
        [jnp.concatenate([mine_ref[at], theirs_ref[at]], axis=1) for at in order], axis=0
    )
    for step in range(steps):
        for half in range(CORES):
            fetch(step, half).wait()
        part = jnp.dot(left, weight[step], preferred_element_type=F32).astype(BF16)
        for hop, out_ref in enumerate(out_refs):
            out_ref[:, step * tile : (step + 1) * tile] = part[hop * rows : (hop + 1) * rows, :]


def project(level, mine, theirs, own, pair):
    depth, rows, width = mine.shape
    wide = own.shape[1]
    tile = 512
    return pl.pallas_call(
        project_kernel,
        in_specs=[SMEM, VMEM, VMEM, HBM, HBM],
        out_specs=[VMEM] * depth,
        out_shape=[jax.ShapeDtypeStruct((rows, wide), BF16)] * depth,
        scratch_shapes=[
            pltpu.VMEM((wide // tile, CORES * width, tile), BF16),
            pltpu.SemaphoreType.DMA((wide // tile, CORES)),
        ],
        compiler_params=room(8),
        cost_estimate=cost(4 * depth * rows * width * wide, 4 * width * wide + 2 * depth * rows * wide),
        name="project",
    )(level, mine, theirs, own, pair)


def prepare_kernel(own, peers, slots, me_ref, x_ref, scale_ref, index_ref, gain_ref, logit_ref, block_ref, *out_refs):
    rows, width = x_ref.shape
    x = x_ref[...].astype(F32)
    inv = lax.rsqrt(jnp.mean(x * x, axis=-1, keepdims=True) + NORM_EPS)
    block_ref[:, :width] = (x * inv * scale_ref[...]).astype(BF16)
    shift = own.bit_length() - 1
    given = [index_ref[...].astype(F32), gain_ref[...], logit_ref[...], jnp.zeros((8 - TOPK - 2, rows), F32)]
    names = jnp.transpose(jnp.concatenate(given, axis=0))
    picks = [names[:, n : n + 1].astype(jnp.int32) for n in range(TOPK)]
    gain, logit = names[:, TOPK : TOPK + 1], names[:, TOPK + 1 : TOPK + 2]
    home = [lax.shift_right_logical(x, jnp.full_like(x, shift)) for x in picks]
    place = [x & (own - 1) for x in picks]
    lane = lax.broadcasted_iota(jnp.int32, (rows, META), 1)
    member = jnp.where((lane == home[0]) | (lane == home[1]), 1.0, 0.0).astype(BF16)
    ti = lax.broadcasted_iota(jnp.int32, (rows, rows), 0)
    tj = lax.broadcasted_iota(jnp.int32, (rows, rows), 1)
    before = jnp.where(ti > tj, 1.0, 0.0).astype(BF16)
    count = jnp.dot(before, member, preferred_element_type=F32)
    rank = [jnp.sum(jnp.where(lane == x, count, 0.0), axis=1, keepdims=True) for x in home]
    lead = jax.nn.sigmoid(logit)
    mixing = [gain * lead, gain * (1.0 - lead)]
    high = [x.astype(BF16).astype(F32) for x in mixing]
    low = [x - y for x, y in zip(mixing, high)]
    columns = [x.astype(F32) for x in home] + rank + [x.astype(F32) for x in place] + high + low
    meta = jnp.zeros((rows, META), F32)
    for number, column in enumerate(columns):
        meta = jnp.where(lane == number, column, meta)
    block_ref[:, width:] = meta.astype(BF16)
    dispatch_kernel(peers, slots, me_ref, block_ref, *out_refs)


def prepare(own, peers, slots, me, tokens, scale, index, weight, logit):
    rows, width = tokens.shape
    inputs = (tokens, scale.reshape(1, -1), index.T, weight.reshape(1, -1), logit.reshape(1, -1))
    full = lambda *shape: pl.BlockSpec(shape, lambda x: (0,) * len(shape))
    block = jax.ShapeDtypeStruct((rows, width + META), BF16)
    return pl.pallas_call(
        functools.partial(prepare_kernel, own, peers, slots),
        grid=(1,),
        in_specs=[SMEM] + [full(*x.shape) for x in inputs],
        out_specs=[full(rows, width + META)] + [full(slots, width + META)] * peers,
        out_shape=[block] + [jax.ShapeDtypeStruct((slots, width + META), BF16)] * peers,
        cost_estimate=cost(2 * peers * slots * rows * width, rows * width * 8),
        name="prepare",
    )(me, *inputs)


def placement(me, meta, total, slots):
    rows = meta.shape[0]
    lane = lax.broadcasted_iota(jnp.int32, (rows, total), 1)
    home = [meta[:, x : x + 1].astype(jnp.int32) for x in (0, 1)]
    rank = [meta[:, x : x + 1].astype(jnp.int32) for x in (2, 3)]
    spot = [(x ^ me) * slots + y for x, y in zip(home, rank)]
    return jnp.where((lane == spot[0]) | (lane == spot[1]), 1.0, 0.0)


def dispatch_kernel(peers, slots, me_ref, block_ref, *out_refs):
    width = block_ref.shape[1] - META
    meta = block_ref[:, width:].astype(F32)
    pick = jnp.transpose(placement(me_ref[0], meta, peers * slots, slots)).astype(BF16)
    for number, out_ref in enumerate(out_refs):
        part = pick[number * slots : (number + 1) * slots, :]
        out_ref[...] = jnp.dot(part, block_ref[...], preferred_element_type=F32).astype(BF16)


def dispatch(peers, slots, me, block):
    rows, width = block.shape
    return pl.pallas_call(
        functools.partial(dispatch_kernel, peers, slots),
        in_specs=[SMEM, VMEM],
        out_specs=[VMEM] * peers,
        out_shape=[jax.ShapeDtypeStruct((slots, width), BF16)] * peers,
        compiler_params=room(8),
        cost_estimate=cost(2 * peers * slots * rows * width, (rows + peers * slots) * width * 2),
        name="dispatch",
    )(me, block)


def expert_kernel(moved, peers, slots, me_ref, *refs):
    x_refs, refs = refs[:peers], refs[peers:]
    sources, out_refs = refs[:6], refs[6 : 6 + peers]
    x_all, hidden, held, ready = refs[6 + peers :]
    kept = [held.at[moved.index(x)] if x in moved else sources[x] for x in range(6)]
    own, half, width = sources[0].shape
    units = 2 * half
    rows = peers * slots
    tile = 512

    def fetch(which, expert):
        return pltpu.make_async_copy(
            sources[which].at[expert], kept[which].at[expert], ready.at[which, expert]
        )

    inner_moved = [x for x in moved if x < 4]
    outer_moved = [x for x in moved if x >= 4]
    for whiches in (inner_moved, outer_moved):
        for expert in range(own):
            for which in whiches:
                fetch(which, expert).start()
    for number, x_ref in enumerate(x_refs):
        x_all[number * slots : (number + 1) * slots, :] = x_ref[...]
    meta = x_all[:, width:].astype(F32)
    me = me_ref[0].astype(F32)

    def inward(expert, carry):
        for which in inner_moved:
            fetch(which, expert).wait()
        here = expert.astype(F32)
        weight = jnp.zeros((rows, 1), F32)
        for choice in range(TOPK):
            fits = (meta[:, choice : choice + 1] == me) & (meta[:, 4 + choice : 5 + choice] == here)
            value = meta[:, 6 + choice : 7 + choice] + meta[:, 8 + choice : 9 + choice]
            weight = weight + jnp.where(fits, value, 0.0)
        inner = jnp.concatenate([kept[x][expert] for x in range(4)], axis=0)
        both = lax.dot_general(
            x_all[:, :width], inner, (((1,), (1,)), ((), ())), preferred_element_type=F32
        )
        gating, upward = both[:, :units], both[:, units:]
        hidden[expert] = (gating / (1.0 + jnp.exp(-gating)) * upward * weight).astype(BF16)
        return carry

    lax.fori_loop(0, own, inward, 0)
    for expert in range(own):
        for which in outer_moved:
            fetch(which, expert).wait()

    def outward(step, carry):
        span = pl.ds(pl.multiple_of(step * tile, tile), tile)
        left = jnp.concatenate([hidden[x] for x in range(own)], axis=1)
        right = jnp.concatenate([kept[y][x, :, span] for x in range(own) for y in (4, 5)], axis=0)
        part = jnp.dot(left, right, preferred_element_type=F32).astype(BF16)
        for number, out_ref in enumerate(out_refs):
            out_ref[:, span] = part[number * slots : (number + 1) * slots, :]
        return carry

    lax.fori_loop(0, width // tile, outward, 0)


def expert_part(first, peers, slots, me, arrived, weights):
    own, units, width = weights[0].shape[-3:]
    rows = peers * slots
    moved = tuple(range(6)) if first else (1, 3, 5)
    return pl.pallas_call(
        functools.partial(expert_kernel, moved, peers, slots),
        in_specs=[SMEM] + [VMEM] * peers + [HBM if x in moved else VMEM for x in range(6)],
        out_specs=[VMEM] * peers,
        out_shape=[jax.ShapeDtypeStruct((slots, width), BF16)] * peers,
        scratch_shapes=[
            pltpu.VMEM((rows, width + META), BF16),
            pltpu.VMEM((own, rows, 2 * units), BF16),
            pltpu.VMEM((len(moved), own, units, width), BF16),
            pltpu.SemaphoreType.DMA((6, own)),
        ],
        compiler_params=pltpu.CompilerParams(vmem_limit_bytes=FIRST_ROOM if first else EXPERT_ROOM),
        cost_estimate=cost(12 * own * units * rows * width, 12 * own * units * width + 4 * rows * width),
        name="expert_part",
    )(me, *arrived, *weights)


def collect_kernel(peers, slots, me_ref, meta_ref, *refs):
    pick = placement(me_ref[0], meta_ref[...].astype(F32), peers * slots, slots).astype(BF16)
    back = jnp.concatenate([x[...] for x in refs[:peers]], axis=0)
    found = jnp.dot(pick, back, preferred_element_type=F32)
    for extra in refs[peers:-1]:
        found = found + extra[...].astype(F32)
    refs[-1][...] = found.astype(BF16)


def collect(peers, slots, me, block, returned, extra):
    rows = block.shape[0]
    width = block.shape[1] - META
    full = lambda *shape: pl.BlockSpec(shape, lambda x: (0,) * len(shape))
    return pl.pallas_call(
        functools.partial(collect_kernel, peers, slots),
        grid=(1,),
        in_specs=[SMEM, pl.BlockSpec((rows, META), lambda x: (0, width // META))]
        + [full(slots, width)] * peers
        + [full(rows, width)] * len(extra),
        out_specs=full(rows, width),
        out_shape=jax.ShapeDtypeStruct((rows, width), BF16),
        compiler_params=room(8),
        cost_estimate=cost(2 * rows * peers * slots * width, (2 * rows + peers * slots) * width * 2),
        name="collect",
    )(me, block, *returned, *extra)


def shards(
    query_heads_rows,
    key_heads_rows,
    value_heads_rows,
    write_strength_logit,
    decay_preactivation,
    head_decay_logarithm,
    extra_log_decay,
    output_weight,
    second_batch_tokens,
    expert_norm_scale,
    expert_choice_index,
    group_router_weight,
    expert_logit_difference,
    expert_gate_weight,
    expert_up_weight,
    expert_down_weight,
):
    ep, tp = lax.axis_size("ep"), lax.axis_size("tp")
    depth = tp // CORES
    me = lax.axis_index("ep")
    rank = lax.axis_index("tp")
    level, core = rank // CORES, rank % CORES
    pair = [(x, x ^ 1) for x in range(tp)]

    def swap(x):
        return lax.ppermute(x, "tp", pair)

    def send(x, chips):
        return lax.ppermute(x, "tp", [(y, (y + chips * CORES) % tp) for y in range(tp)])

    def trade(x, distance):
        return lax.ppermute(x, "ep", [(y, y ^ distance) for y in range(ep)])

    def scalar(x):
        return x.astype(jnp.int32).reshape(1)

    me1 = scalar(me)
    own = EXPERTS // ep
    tokens = second_batch_tokens.shape[0]
    slots = own * CAP // TOPK if own % EPG == 0 else min(own * CAP, tokens)

    block, *sent = prepare(
        own,
        ep,
        slots,
        me1,
        second_batch_tokens,
        expert_norm_scale,
        expert_choice_index,
        group_router_weight,
        expert_logit_difference,
    )
    blocks, arrived = [block], []

    def move(hop):
        return send(blocks[hop - 1], 1)

    def exchange(sent):
        return [sent[0]] + [trade(sent[x], x) for x in range(1, ep)]

    def give_back(produced):
        return [produced[0]] + [trade(produced[x], x) for x in range(1, ep)]

    weights = []
    for shard in (expert_gate_weight, expert_up_weight, expert_down_weight):
        weights += [shard, swap(shard)]
    out_pair = swap(output_weight)

    for hop in range(depth):
        if hop > 0:
            blocks.append(move(hop))
            sent = dispatch(ep, slots, me1, blocks[hop])
        arrived.append(exchange(sent))

    heads = head_decay_logarithm.shape[0]
    local, proj, ends = [], [], []
    for head in range(heads):
        x, y, end = mixer_local(
            head,
            head_decay_logarithm,
            query_heads_rows,
            key_heads_rows,
            value_heads_rows,
            write_strength_logit,
            decay_preactivation,
            extra_log_decay,
            ends if head == heads - 1 else [],
        )
        local.append(x)
        proj.append(y)
        ends.append(end)
    joint = ends[-1]
    joint, weights = lax.optimization_barrier((joint, weights))
    eye = jnp.concatenate([jnp.zeros((DK, DV), F32), jnp.eye(DK, dtype=F32)], axis=1)
    inner = jnp.broadcast_to(eye, joint.shape)
    span = 1
    while True:
        late = scalar((me // span) % 2)
        final = 2 * span >= ep
        got = trade(joint[..., :DV] if final else joint, span)
        if final:
            break
        joint, inner = join(late, joint, got, inner)
        span *= 2
    mine, other = attend(depth, late, scalar(core), local, proj, got, inner)
    theirs = swap(other)
    pieces = project(scalar(level), mine, theirs, output_weight, out_pair)

    mixed = pieces[0].astype(F32)
    for hop in range(1, depth):
        mixed = mixed + send(pieces[hop], -hop).astype(F32)

    found = {}
    for hop in list(range(1, depth)) + [0]:
        produced = expert_part(hop in FETCH, ep, slots, me1, arrived[hop], weights)
        found[hop] = give_back(produced)
    running, near = [], []
    for hop in range(1, depth):
        total = collect(ep, slots, me1, blocks[hop], found[hop], running)
        if hop == 1:
            near = [send(total, -1)]
        else:
            running = [send(total, 1)]
    expert_out = collect(ep, slots, me1, blocks[0], found[0], near)
    if running:
        expert_out = (expert_out.astype(F32) + running[0].astype(F32)).astype(BF16)
    return (mixed.astype(BF16), expert_out)


def solution(mesh):
    in_specs = (
        P("ep", "tp"),
        P("ep", "tp"),
        P("ep", "tp"),
        P("tp", "ep"),
        P("tp", "ep"),
        P("tp"),
        P("tp", "ep"),
        P("tp", None),
        P(("ep", "tp"), None),
        P(),
        P(("ep", "tp"), None),
        P(("ep", "tp")),
        P(("ep", "tp")),
        P("ep", "tp", None),
        P("ep", "tp", None),
        P("ep", "tp", None),
    )
    out_specs = (P(("ep", "tp"), None), P(("ep", "tp"), None))

    return jax.shard_map(shards, mesh=mesh, in_specs=in_specs, out_specs=out_specs, check_vma=False)
```

```python
import functools

import jax
import jax.numpy as jnp
from jax import lax
from jax.experimental import pallas as pl
from jax.experimental.pallas import tpu as pltpu
from jax.sharding import PartitionSpec as P


DK = 128
DV = 128
CAP = 32
EXPERTS = 16
EPG = 4
TOPK = 2
CORES = 2
META = 128
CHUNK = 128
FIRST_ROOM, EXPERT_ROOM = 64000 * 1024, 24 * 2**20
FETCH = (1,)
NORM_EPS = 1e-06


F32 = jnp.float32
BF16 = jnp.bfloat16
EXACT = lax.Precision.HIGHEST
VMEM = pl.BlockSpec(memory_space=pltpu.VMEM)
HBM = pl.BlockSpec(memory_space=pltpu.HBM)
SMEM = pl.BlockSpec(memory_space=pltpu.SMEM)


def room(mib):
    return pltpu.CompilerParams(vmem_limit_bytes=mib * 2**20)


def cost(flops, moved):
    return pl.CostEstimate(flops=int(flops), bytes_accessed=int(moved), transcendentals=0)


def mm(a, b):
    return jnp.dot(a, b, precision=EXACT, preferred_element_type=F32)


def halves(x):
    high = x.astype(BF16)
    return high, (x - high.astype(F32)).astype(BF16)


def mm3(a, b):
    (ah, al), (bh, bl) = halves(a), halves(b)
    dot = lambda x, y: jnp.dot(x, y, preferred_element_type=F32)
    return dot(ah, bh) + (dot(ah, bl) + dot(al, bh))


def mixer_kernel(head, rate_ref, q_ref, k_ref, v_ref, write_ref, decay_ref, extra_ref, *refs):
    early_refs, (local_ref, proj_ref, joint_ref) = refs[:-3], refs[-3:]
    length = q_ref.shape[0]
    chunks = length // CHUNK
    i = lax.broadcasted_iota(jnp.int32, (CHUNK, CHUNK), 0)
    j = lax.broadcasted_iota(jnp.int32, (CHUNK, CHUNK), 1)
    every = range(chunks)
    spans = [slice(c * CHUNK, (c + 1) * CHUNK) for c in every]

    def unit(ref, n):
        x = ref[spans[n], :].astype(F32)
        return x * lax.rsqrt(jnp.sum(x * x, axis=-1, keepdims=True) + NORM_EPS)

    q = [unit(q_ref, n) * DK**-0.5 for n in every]
    k = [unit(k_ref, n) for n in every]
    kt = [jnp.transpose(x) for x in k]
    v = [v_ref[spans[n], :].astype(F32) for n in every]
    raised = decay_ref[head : head + 1, :].astype(F32)
    soft = jnp.maximum(raised, 0.0) + jnp.log(1.0 + jnp.exp(-jnp.abs(raised)))
    rate = jnp.exp(jnp.full((1, length), rate_ref[head], F32))
    drops = extra_ref[head : head + 1, :] - rate * soft
    writes = jax.nn.sigmoid(write_ref[head : head + 1, :].astype(F32))
    drops = jnp.concatenate([drops[:, x] for x in spans], axis=0)
    writes = jnp.concatenate([writes[:, x] for x in spans], axis=0)
    summed = mm(drops, jnp.where(i <= j, 1.0, 0.0))
    columns = jnp.transpose(jnp.concatenate([summed, writes], axis=0))
    row = [summed[n : n + 1, :] for n in every]
    col = [columns[:, n : n + 1] for n in every]
    beta = [columns[:, len(every) + n : len(every) + n + 1] for n in every]
    last = [r[:, CHUNK - 1 :] for r in row]
    decay = [jnp.where(i >= j, jnp.exp(jnp.where(i >= j, col[n] - row[n], 0.0)), 0.0) for n in every]
    gram = [mm3(k[n], kt[n]) for n in every]
    lower = [jnp.where(i > j, gram[n] * decay[n] * beta[n], 0.0) for n in every]
    scores = [mm3(q[n], kt[n]) * decay[n] for n in every]
    eye = jnp.where(i == j, 1.0, 0.0)
    small = 16
    near = (i // small) == (j // small)
    power = [jnp.where(near, x, 0.0) for x in lower]
    inverse = [eye - x for x in power]
    reach = 2
    while reach < small:
        power = [mm3(x, x) for x in power]
        inverse = [x + mm3(x, y) for x, y in zip(inverse, power)]
        reach *= 2
    while small < CHUNK:
        band = ((i // (2 * small)) == (j // (2 * small))) & ((i // small) != (j // small))
        half = [mm3(jnp.where(band, x, 0.0), y) for x, y in zip(lower, inverse)]
        inverse = [y - mm3(y, x) for x, y in zip(half, inverse)]
        small *= 2
    grown = [jnp.exp(x) for x in col]
    rhs = [jnp.concatenate([v[n] * beta[n], k[n] * (beta[n] * grown[n])], axis=1) for n in every]
    solved = [mm3(inverse[n], rhs[n]) for n in every]
    blank = jnp.zeros((CHUNK, DK), F32)
    start = jnp.concatenate([jnp.zeros((DK, DV), F32), eye], axis=1)
    joint = start
    for n in every:
        update = jnp.concatenate([solved[n][:, :DV], blank], axis=1) - mm3(solved[n][:, DV:], joint)
        out = mm3(q[n] * grown[n], joint) + mm3(scores[n], update)
        joint = joint * jnp.exp(last[n]) + mm3(kt[n] * jnp.exp(last[n] - row[n]), update)
        local_ref[spans[n], :] = out[:, :DV]
        proj_ref[spans[n], :] = out[:, DV:].astype(BF16)
    for number, early_ref in enumerate(early_refs):
        joint_ref[number] = early_ref[0]
    joint_ref[len(early_refs)] = joint


def mixer_local(head, rates, queries, keys, values, write, decay, extra, early):
    length = queries.shape[0]
    tall = pl.BlockSpec((length, DK), lambda x: (0, head))
    gate = pl.BlockSpec(write.shape, lambda x: (0, 0))
    flat = pl.BlockSpec((length, DK), lambda x: (0, 0))
    ends = lambda n: pl.BlockSpec((n, DK, DV + DK), lambda x: (0, 0, 0))
    return pl.pallas_call(
        functools.partial(mixer_kernel, head),
        grid=(1,),
        in_specs=[SMEM] + [tall] * 3 + [gate] * 3 + [ends(1)] * len(early),
        out_specs=[flat, flat, ends(1 + len(early))],
        out_shape=[
            jax.ShapeDtypeStruct((length, DV), F32),
            jax.ShapeDtypeStruct((length, DK), BF16),
            jax.ShapeDtypeStruct((1 + len(early), DK, DV + DK), F32),
        ],
        cost_estimate=cost(length // CHUNK * 26 * 6 * 2 * 128**3, length * DK * 14),
        name="mixer_local",
    )(rates, queries, keys, values, write, decay, extra, *early)


def join_kernel(late_ref, own_ref, got_ref, inner_ref, own_out, inner_out):
    late = late_ref[0] > 0
    for h in range(own_ref.shape[0]):
        own, got, inner = own_ref[h], got_ref[h].astype(F32), inner_ref[h]
        first, second = jnp.where(late, got, own), jnp.where(late, own, got)
        blank = jnp.zeros_like(own[:, DV:])
        keep = lambda x: jnp.concatenate([x[:, :DV], blank], axis=1)
        own_out[h] = mm(second[:, DV:], first) + keep(second)
        inner_out[h] = jnp.where(late, mm(inner[:, DV:], got) + keep(inner), inner)


def join(late, own, got, inner):
    shape = jax.ShapeDtypeStruct(own.shape, F32)
    return pl.pallas_call(
        join_kernel,
        in_specs=[SMEM] + [VMEM] * 3,
        out_specs=[VMEM] * 2,
        out_shape=[shape, shape],
        compiler_params=room(8),
        cost_estimate=cost(own.size * 24 * DK, own.size * 20),
        name="join",
    )(late, own, got, inner)


def attend_kernel(heads, late_ref, core_ref, *refs):
    local_refs, proj_refs = refs[:heads], refs[heads : 2 * heads]
    got_ref, inner_ref, mine_ref, other_ref = refs[2 * heads :]
    late = late_ref[0] > 0
    states = []
    for h in range(heads):
        inner = inner_ref[h]
        state = mm3(inner[:, DV:], got_ref[h].astype(F32)) + inner[:, :DV]
        states.append(jnp.concatenate(halves(jnp.where(late, state, inner[:, :DV])), axis=1))
    depth, rows = mine_ref.shape[0], mine_ref.shape[1]
    for out_ref, shift in ((mine_ref, core_ref[0]), (other_ref, 1 - core_ref[0])):
        for z in range(depth):
            span = pl.ds(pl.multiple_of((z * CORES + shift) * rows, rows), rows)
            for h in range(heads):
                both = jnp.dot(proj_refs[h][span, :], states[h], preferred_element_type=F32)
                out = local_refs[h][span, :] + both[:, :DV] + both[:, DV:]
                out_ref[z, :, h * DV : (h + 1) * DV] = out.astype(BF16)


def attend(depth, late, core, local, proj, got, inner):
    heads = len(local)
    length, width = local[0].shape
    half = jax.ShapeDtypeStruct((depth, length // depth // CORES, heads * width), BF16)
    full = lambda *shape: pl.BlockSpec(shape, lambda x: (0,) * len(shape))
    return pl.pallas_call(
        functools.partial(attend_kernel, heads),
        grid=(1,),
        in_specs=[SMEM] * 2 + [full(length, width)] * (2 * heads) + [full(*got.shape), full(*inner.shape)],
        out_specs=[full(*half.shape)] * 2,
        out_shape=[half, half],
        cost_estimate=cost(6 * 2 * length * width * DK * heads, length * width * 10 * heads),
        name="attend",
    )(late, core, *local, *proj, got, inner)


def project_kernel(level_ref, mine_ref, theirs_ref, own_ref, pair_ref, *refs):
    depth, rows, width = mine_ref.shape
    out_refs, (weight, ready) = refs[:depth], refs[depth:]
    tile = weight.shape[2]
    steps = weight.shape[0]

    def fetch(step, half):
        source = (own_ref, pair_ref)[half]
        return pltpu.make_async_copy(
            source.at[:, pl.ds(step * tile, tile)],
            weight.at[step, pl.ds(half * width, width)],
            ready.at[step, half],
        )

    for step in range(steps):
        for half in range(CORES):
            fetch(step, half).start()
    order = [lax.rem(level_ref[0] + depth - hop, depth) for hop in range(depth)]
    left = jnp.concatenate(
        [jnp.concatenate([mine_ref[at], theirs_ref[at]], axis=1) for at in order], axis=0
    )
    for step in range(steps):
        for half in range(CORES):
            fetch(step, half).wait()
        part = jnp.dot(left, weight[step], preferred_element_type=F32).astype(BF16)
        for hop, out_ref in enumerate(out_refs):
            out_ref[:, step * tile : (step + 1) * tile] = part[hop * rows : (hop + 1) * rows, :]


def project(level, mine, theirs, own, pair):
    depth, rows, width = mine.shape
    wide = own.shape[1]
    tile = 512
    return pl.pallas_call(
        project_kernel,
        in_specs=[SMEM, VMEM, VMEM, HBM, HBM],
        out_specs=[VMEM] * depth,
        out_shape=[jax.ShapeDtypeStruct((rows, wide), BF16)] * depth,
        scratch_shapes=[
            pltpu.VMEM((wide // tile, CORES * width, tile), BF16),
            pltpu.SemaphoreType.DMA((wide // tile, CORES)),
        ],
        compiler_params=room(8),
        cost_estimate=cost(4 * depth * rows * width * wide, 4 * width * wide + 2 * depth * rows * wide),
        name="project",
    )(level, mine, theirs, own, pair)


def prepare_kernel(own, peers, slots, me_ref, x_ref, scale_ref, index_ref, gain_ref, logit_ref, block_ref, *out_refs):
    rows, width = x_ref.shape
    x = x_ref[...].astype(F32)
    inv = lax.rsqrt(jnp.mean(x * x, axis=-1, keepdims=True) + NORM_EPS)
    block_ref[:, :width] = (x * inv * scale_ref[...]).astype(BF16)
    shift = own.bit_length() - 1
    given = [index_ref[...].astype(F32), gain_ref[...], logit_ref[...], jnp.zeros((8 - TOPK - 2, rows), F32)]
    names = jnp.transpose(jnp.concatenate(given, axis=0))
    picks = [names[:, n : n + 1].astype(jnp.int32) for n in range(TOPK)]
    gain, logit = names[:, TOPK : TOPK + 1], names[:, TOPK + 1 : TOPK + 2]
    home = [lax.shift_right_logical(x, jnp.full_like(x, shift)) for x in picks]
    place = [x & (own - 1) for x in picks]
    lane = lax.broadcasted_iota(jnp.int32, (rows, META), 1)
    member = jnp.where((lane == home[0]) | (lane == home[1]), 1.0, 0.0).astype(BF16)
    ti = lax.broadcasted_iota(jnp.int32, (rows, rows), 0)
    tj = lax.broadcasted_iota(jnp.int32, (rows, rows), 1)
    before = jnp.where(ti > tj, 1.0, 0.0).astype(BF16)
    count = jnp.dot(before, member, preferred_element_type=F32)
    rank = [jnp.sum(jnp.where(lane == x, count, 0.0), axis=1, keepdims=True) for x in home]
    lead = jax.nn.sigmoid(logit)
    mixing = [gain * lead, gain * (1.0 - lead)]
    high = [x.astype(BF16).astype(F32) for x in mixing]
    low = [x - y for x, y in zip(mixing, high)]
    columns = [x.astype(F32) for x in home] + rank + [x.astype(F32) for x in place] + high + low
    meta = jnp.zeros((rows, META), F32)
    for number, column in enumerate(columns):
        meta = jnp.where(lane == number, column, meta)
    block_ref[:, width:] = meta.astype(BF16)
    dispatch_kernel(peers, slots, me_ref, block_ref, *out_refs)


def prepare(own, peers, slots, me, tokens, scale, index, weight, logit):
    rows, width = tokens.shape
    inputs = (tokens, scale.reshape(1, -1), index.T, weight.reshape(1, -1), logit.reshape(1, -1))
    full = lambda *shape: pl.BlockSpec(shape, lambda x: (0,) * len(shape))
    block = jax.ShapeDtypeStruct((rows, width + META), BF16)
    return pl.pallas_call(
        functools.partial(prepare_kernel, own, peers, slots),
        grid=(1,),
        in_specs=[SMEM] + [full(*x.shape) for x in inputs],
        out_specs=[full(rows, width + META)] + [full(slots, width + META)] * peers,
        out_shape=[block] + [jax.ShapeDtypeStruct((slots, width + META), BF16)] * peers,
        cost_estimate=cost(2 * peers * slots * rows * width, rows * width * 8),
        name="prepare",
    )(me, *inputs)


def placement(me, meta, total, slots):
    rows = meta.shape[0]
    lane = lax.broadcasted_iota(jnp.int32, (rows, total), 1)
    home = [meta[:, x : x + 1].astype(jnp.int32) for x in (0, 1)]
    rank = [meta[:, x : x + 1].astype(jnp.int32) for x in (2, 3)]
    spot = [(x ^ me) * slots + y for x, y in zip(home, rank)]
    return jnp.where((lane == spot[0]) | (lane == spot[1]), 1.0, 0.0)


def dispatch_kernel(peers, slots, me_ref, block_ref, *out_refs):
    width = block_ref.shape[1] - META
    meta = block_ref[:, width:].astype(F32)
    pick = jnp.transpose(placement(me_ref[0], meta, peers * slots, slots)).astype(BF16)
    for number, out_ref in enumerate(out_refs):
        part = pick[number * slots : (number + 1) * slots, :]
        out_ref[...] = jnp.dot(part, block_ref[...], preferred_element_type=F32).astype(BF16)


def dispatch(peers, slots, me, block):
    rows, width = block.shape
    return pl.pallas_call(
        functools.partial(dispatch_kernel, peers, slots),
        in_specs=[SMEM, VMEM],
        out_specs=[VMEM] * peers,
        out_shape=[jax.ShapeDtypeStruct((slots, width), BF16)] * peers,
        compiler_params=room(8),
        cost_estimate=cost(2 * peers * slots * rows * width, (rows + peers * slots) * width * 2),
        name="dispatch",
    )(me, block)


def expert_kernel(moved, peers, slots, me_ref, *refs):
    x_refs, refs = refs[:peers], refs[peers:]
    sources, out_refs = refs[:6], refs[6 : 6 + peers]
    x_all, hidden, held, ready = refs[6 + peers :]
    kept = [held.at[moved.index(x)] if x in moved else sources[x] for x in range(6)]
    own, half, width = sources[0].shape
    units = 2 * half
    rows = peers * slots
    tile = 512

    def fetch(which, expert):
        return pltpu.make_async_copy(
            sources[which].at[expert], kept[which].at[expert], ready.at[which, expert]
        )

    inner_moved = [x for x in moved if x < 4]
    outer_moved = [x for x in moved if x >= 4]
    for whiches in (inner_moved, outer_moved):
        for expert in range(own):
            for which in whiches:
                fetch(which, expert).start()
    for number, x_ref in enumerate(x_refs):
        x_all[number * slots : (number + 1) * slots, :] = x_ref[...]
    meta = x_all[:, width:].astype(F32)
    me = me_ref[0].astype(F32)

    def inward(expert, carry):
        for which in inner_moved:
            fetch(which, expert).wait()
        here = expert.astype(F32)
        weight = jnp.zeros((rows, 1), F32)
        for choice in range(TOPK):
            fits = (meta[:, choice : choice + 1] == me) & (meta[:, 4 + choice : 5 + choice] == here)
            value = meta[:, 6 + choice : 7 + choice] + meta[:, 8 + choice : 9 + choice]
            weight = weight + jnp.where(fits, value, 0.0)
        inner = jnp.concatenate([kept[x][expert] for x in range(4)], axis=0)
        both = lax.dot_general(
            x_all[:, :width], inner, (((1,), (1,)), ((), ())), preferred_element_type=F32
        )
        gating, upward = both[:, :units], both[:, units:]
        hidden[expert] = (gating / (1.0 + jnp.exp(-gating)) * upward * weight).astype(BF16)
        return carry

    lax.fori_loop(0, own, inward, 0)
    for expert in range(own):
        for which in outer_moved:
            fetch(which, expert).wait()

    def outward(step, carry):
        span = pl.ds(pl.multiple_of(step * tile, tile), tile)
        left = jnp.concatenate([hidden[x] for x in range(own)], axis=1)
        right = jnp.concatenate([kept[y][x, :, span] for x in range(own) for y in (4, 5)], axis=0)
        part = jnp.dot(left, right, preferred_element_type=F32).astype(BF16)
        for number, out_ref in enumerate(out_refs):
            out_ref[:, span] = part[number * slots : (number + 1) * slots, :]
        return carry

    lax.fori_loop(0, width // tile, outward, 0)


def expert_part(first, peers, slots, me, arrived, weights):
    own, units, width = weights[0].shape[-3:]
    rows = peers * slots
    moved = tuple(range(6)) if first else (1, 3, 5)
    return pl.pallas_call(
        functools.partial(expert_kernel, moved, peers, slots),
        in_specs=[SMEM] + [VMEM] * peers + [HBM if x in moved else VMEM for x in range(6)],
        out_specs=[VMEM] * peers,
        out_shape=[jax.ShapeDtypeStruct((slots, width), BF16)] * peers,
        scratch_shapes=[
            pltpu.VMEM((rows, width + META), BF16),
            pltpu.VMEM((own, rows, 2 * units), BF16),
            pltpu.VMEM((len(moved), own, units, width), BF16),
            pltpu.SemaphoreType.DMA((6, own)),
        ],
        compiler_params=pltpu.CompilerParams(vmem_limit_bytes=FIRST_ROOM if first else EXPERT_ROOM),
        cost_estimate=cost(12 * own * units * rows * width, 12 * own * units * width + 4 * rows * width),
        name="expert_part",
    )(me, *arrived, *weights)


def collect_kernel(peers, slots, me_ref, meta_ref, *refs):
    pick = placement(me_ref[0], meta_ref[...].astype(F32), peers * slots, slots).astype(BF16)
    back = jnp.concatenate([x[...] for x in refs[:peers]], axis=0)
    found = jnp.dot(pick, back, preferred_element_type=F32)
    for extra in refs[peers:-1]:
        found = found + extra[...].astype(F32)
    refs[-1][...] = found.astype(BF16)


def collect(peers, slots, me, block, returned, extra):
    rows = block.shape[0]
    width = block.shape[1] - META
    full = lambda *shape: pl.BlockSpec(shape, lambda x: (0,) * len(shape))
    return pl.pallas_call(
        functools.partial(collect_kernel, peers, slots),
        grid=(1,),
        in_specs=[SMEM, pl.BlockSpec((rows, META), lambda x: (0, width // META))]
        + [full(slots, width)] * peers
        + [full(rows, width)] * len(extra),
        out_specs=full(rows, width),
        out_shape=jax.ShapeDtypeStruct((rows, width), BF16),
        compiler_params=room(8),
        cost_estimate=cost(2 * rows * peers * slots * width, (2 * rows + peers * slots) * width * 2),
        name="collect",
    )(me, block, *returned, *extra)


def shards(
    query_heads_rows,
    key_heads_rows,
    value_heads_rows,
    write_strength_logit,
    decay_preactivation,
    head_decay_logarithm,
    extra_log_decay,
    output_weight,
    second_batch_tokens,
    expert_norm_scale,
    expert_choice_index,
    group_router_weight,
    expert_logit_difference,
    expert_gate_weight,
    expert_up_weight,
    expert_down_weight,
):
    ep, tp = lax.axis_size("ep"), lax.axis_size("tp")
    depth = tp // CORES
    me = lax.axis_index("ep")
    rank = lax.axis_index("tp")
    level, core = rank // CORES, rank % CORES
    pair = [(x, x ^ 1) for x in range(tp)]

    def swap(x):
        return lax.ppermute(x, "tp", pair)

    def send(x, chips):
        return lax.ppermute(x, "tp", [(y, (y + chips * CORES) % tp) for y in range(tp)])

    def trade(x, distance):
        return lax.ppermute(x, "ep", [(y, y ^ distance) for y in range(ep)])

    def scalar(x):
        return x.astype(jnp.int32).reshape(1)

    me1 = scalar(me)
    own = EXPERTS // ep
    tokens = second_batch_tokens.shape[0]
    slots = own * CAP // TOPK if own % EPG == 0 else min(own * CAP, tokens)

    block, *sent = prepare(
        own,
        ep,
        slots,
        me1,
        second_batch_tokens,
        expert_norm_scale,
        expert_choice_index,
        group_router_weight,
        expert_logit_difference,
    )
    blocks, arrived = [block], []

    def move(hop):
        return send(blocks[hop - 1], 1)

    def exchange(sent):
        return [sent[0]] + [trade(sent[x], x) for x in range(1, ep)]

    def give_back(produced):
        return [produced[0]] + [trade(produced[x], x) for x in range(1, ep)]

    weights = []
    for shard in (expert_gate_weight, expert_up_weight, expert_down_weight):
        weights += [shard, swap(shard)]
    out_pair = swap(output_weight)

    for hop in range(depth):
        if hop > 0:
            blocks.append(move(hop))
            sent = dispatch(ep, slots, me1, blocks[hop])
        arrived.append(exchange(sent))

    heads = head_decay_logarithm.shape[0]
    local, proj, ends = [], [], []
    for head in range(heads):
        x, y, end = mixer_local(
            head,
            head_decay_logarithm,
            query_heads_rows,
            key_heads_rows,
            value_heads_rows,
            write_strength_logit,
            decay_preactivation,
            extra_log_decay,
            ends if head == heads - 1 else [],
        )
        local.append(x)
        proj.append(y)
        ends.append(end)
    joint = ends[-1]
    joint, weights = lax.optimization_barrier((joint, weights))
    eye = jnp.concatenate([jnp.zeros((DK, DV), F32), jnp.eye(DK, dtype=F32)], axis=1)
    inner = jnp.broadcast_to(eye, joint.shape)
    span = 1
    while True:
        late = scalar((me // span) % 2)
        final = 2 * span >= ep
        got = trade((joint[..., :DV] if final else joint).astype(BF16), span)
        if final:
            break
        joint, inner = join(late, joint, got, inner)
        span *= 2
    mine, other = attend(depth, late, scalar(core), local, proj, got, inner)
    theirs = swap(other)
    pieces = project(scalar(level), mine, theirs, output_weight, out_pair)

    mixed = pieces[0].astype(F32)
    for hop in range(1, depth):
        mixed = mixed + send(pieces[hop], -hop).astype(F32)

    found = {}
    for hop in list(range(1, depth)) + [0]:
        produced = expert_part(hop in FETCH, ep, slots, me1, arrived[hop], weights)
        found[hop] = give_back(produced)
    running, near = [], []
    for hop in range(1, depth):
        total = collect(ep, slots, me1, blocks[hop], found[hop], running)
        if hop == 1:
            near = [send(total, -1)]
        else:
            running = [send(total, 1)]
    expert_out = collect(ep, slots, me1, blocks[0], found[0], near)
    if running:
        expert_out = (expert_out.astype(F32) + running[0].astype(F32)).astype(BF16)
    return (mixed.astype(BF16), expert_out)


def solution(mesh):
    in_specs = (
        P("ep", "tp"),
        P("ep", "tp"),
        P("ep", "tp"),
        P("tp", "ep"),
        P("tp", "ep"),
        P("tp"),
        P("tp", "ep"),
        P("tp", None),
        P(("ep", "tp"), None),
        P(),
        P(("ep", "tp"), None),
        P(("ep", "tp")),
        P(("ep", "tp")),
        P("ep", "tp", None),
        P("ep", "tp", None),
        P("ep", "tp", None),
    )
    out_specs = (P(("ep", "tp"), None), P(("ep", "tp"), None))

    return jax.shard_map(shards, mesh=mesh, in_specs=in_specs, out_specs=out_specs, check_vma=False)
```
